512 devices in a mesh: sp: 64 (over z, y), tp: 8 (over x, core).
Axes of the slice: x: 4, y: 8, z: 8, core: 2. Of those that a mesh axis runs over, the one named last changes fastest.
Arguments:
- inner_pre: bfloat16 [24576, 4096], P('sp', 'tp'), may hold values from -6 to 6
- coeff_pre: bfloat16 [24576, 2, 1024], P('sp', None, 'tp'), may hold values from -6 to 6
- gate_pre: bfloat16 [24576, 4096], P('sp', 'tp'), may hold values from -6 to 6
- step_raw: bfloat16 [24576, 64], P('sp', 'tp'), may hold values from -2.5 to 2.5
- step_bias: float32 [64], P('tp'), may hold values from -3.3 to 0.8
- decay_log: float32 [64], P('tp'), may hold values from -8.5 to -3.5
- conv_inner: bfloat16 [4, 4096], P(None, 'tp'), may hold values from -3 to 3
- conv_coeff: bfloat16 [4, 2, 1024], P(None, None, 'tp'), may hold values from -3 to 3
- mixer_gain: float32 [4096], P('tp'), may hold values from 0.1 to 1.9
- out_weight: bfloat16 [4096, 2048], P('tp'), may hold values from -0.125 to 0.125
- residual: bfloat16 [24576, 2048], P('sp', 'tp'), may hold values from -12 to 12
- mlp_gain: float32 [2048], P('tp'), may hold values from 0.1 to 1.9
- up_weight: bfloat16 [2048, 8192], P('sp', 'tp'), may hold values from -0.125 to 0.125
- down_weight: bfloat16 [8192, 2048], P('tp', 'sp'), may hold values from -0.1875 to 0.1875
Outputs:
- layer_out: bfloat16 [24576, 2048], P('sp', 'tp')
The draws below stay inside these ranges and needn't reach their ends.
All inputs are finite; a program needn't handle non-finite values.
Results may differ from the reference program's by a relative error of at most 0.02.
Values may be sent and summed in bfloat16 or wider, within the bound.
A program may use at most 64 MiB of HBM per device.

```python
import jax
import jax.numpy as jnp
from jax import lax

D = 2048
INNER = 4096
HEAD_DIM = 64
GROUPS = 8
STATE = 128
FF = 8192
CONV_TAPS = 4
BLOCK = 128
HEADS = 64
SEQ = 24576
N_TP = 8


def draw_step_raw(key, part):
    jitter_key, level_key = jax.random.split(key)
    jitter = jnp.clip(0.5 * jax.random.normal(jitter_key, (SEQ, HEADS), jnp.float32), -1.5, 1.5)
    levels = jax.random.uniform(level_key, (SEQ // BLOCK, HEADS), jnp.float32, -1.0, 1.0)
    return (jitter + jnp.repeat(levels, BLOCK, axis=0)).astype(jnp.bfloat16)


def draw_step_bias(key, part):
    slow_key, quick_key = jax.random.split(key)
    parity = jnp.arange(HEADS) % 2 == 0
    slow_bias = jax.random.uniform(slow_key, (HEADS,), jnp.float32, -3.3, -2.7)
    quick_bias = jax.random.uniform(quick_key, (HEADS,), jnp.float32, 0.2, 0.8)
    return jnp.where(parity, slow_bias, quick_bias)


def draw_decay_log(key, part):
    slow_key, quick_key = jax.random.split(key)
    parity = jnp.arange(HEADS) % 2 == 0
    slow_rate = jax.random.uniform(slow_key, (HEADS,), jnp.float32, -8.5, -7.5)
    quick_rate = jax.random.uniform(quick_key, (HEADS,), jnp.float32, -4.6, -3.5)
    return jnp.where(parity, slow_rate, quick_rate)


def draw_residual(key, part):
    base_key = jax.random.fold_in(key, 7)
    noise_key, scale_key = jax.random.split(base_key)
    noise = jnp.clip(jax.random.normal(noise_key, (SEQ, D), jnp.float32), -4.0, 4.0)
    log_scales = jax.random.uniform(scale_key, (SEQ, 16), jnp.float32, jnp.log(0.3), jnp.log(3.0))
    scales = jnp.repeat(jnp.exp(log_scales), D // 16, axis=1)
    return (noise * scales).astype(jnp.bfloat16)


def with_spikes(array, key, source, target, shards_of, factor):
    owner, partner = [(jnp.arange(array.shape[axis_at]) // (array.shape[axis_at] // shards_of)).reshape([-1 if axis == axis_at else 1 for axis in range(array.ndim)]) for axis_at in (source, target)]
    chosen = jax.random.permutation(key, shards_of)[partner]
    strong = (owner == chosen) | (owner == (partner + shards_of // 2) % shards_of)
    return jnp.where(strong, factor * array, array)


def block_scale(stream_key, dims, shards, low, top_value):
    factor_of, own = 1.0, jax.random.fold_in(stream_key, 6)
    for dim, shards_of in shards:
        steps = jnp.exp(jax.random.uniform(jax.random.fold_in(own, dim), (shards_of,), jnp.float32, low / len(shards), top_value / len(shards)))
        factor_of = factor_of * jnp.repeat(steps, dims[dim] // shards_of).reshape([-1 if axis == dim else 1 for axis in range(len(dims))])
    return factor_of


def normal_values(key, dims, width, limit, cuts=(), kind=jnp.bfloat16):
    array = width * jax.random.normal(key, dims, jnp.float32)
    if cuts:
        array = array * block_scale(key, dims, cuts, -0.22, 0.18)
    return jnp.clip(array, -limit, limit).astype(kind)


def noise_with(stream_key, dims, deviation, most, shards, heavy, held_as=jnp.bfloat16):
    entries = deviation * jax.random.normal(stream_key, dims, jnp.float32)
    if shards:
        entries = entries * block_scale(stream_key, dims, shards, -0.22, 0.18)
    return jnp.clip(with_spikes(entries, jax.random.fold_in(stream_key, 3), *heavy), -most, most).astype(held_as)


def setup_inputs(seed: int = 0) -> dict:
    keys = jax.random.split(jax.random.key(seed), 15)
    return {
        "inner_pre": normal_values(keys[0], (SEQ, INNER), 1.0, 6.0, ((0, 64), (1, 8))),
        "coeff_pre": normal_values(keys[1], (SEQ, 2, GROUPS * STATE), 1.0, 6.0, ((0, 64), (2, 8))),
        "gate_pre": normal_values(keys[2], (SEQ, INNER), 1.0, 6.0, ((0, 64), (1, 8))),
        "step_raw": draw_step_raw(jax.random.fold_in(keys[14], 71), 0),
        "step_bias": draw_step_bias(jax.random.fold_in(keys[14], 71), 0),
        "decay_log": draw_decay_log(jax.random.fold_in(keys[14], 71), 0),
        "conv_inner": normal_values(keys[6], (CONV_TAPS, INNER), CONV_TAPS ** -0.5, 3.0, ((1, 8),)),
        "conv_coeff": normal_values(keys[7], (CONV_TAPS, 2, GROUPS * STATE), CONV_TAPS ** -0.5, 3.0, ((2, 8),)),
        "mixer_gain": jnp.clip(1.0 + 0.18 * jax.random.normal(keys[8], (INNER,), jnp.float32), 0.1, 1.9),
        "out_weight": noise_with(keys[9], (INNER, D), INNER ** -0.5, 0.125, ((0, 8),), (0, 1, 8, 2.0)),
        "residual": draw_residual(jax.random.fold_in(keys[14], 71), 0),
        "mlp_gain": jnp.clip(1.0 + 0.18 * jax.random.normal(keys[11], (D,), jnp.float32), 0.1, 1.9),
        "up_weight": normal_values(keys[12], (D, FF), D ** -0.5, 0.125, ((0, 64), (1, 8))),
        "down_weight": noise_with(keys[13], (FF, D), FF ** -0.5, 0.1875, ((0, 8), (1, 64)), (0, 1, 64, 4.0)),
    }


eps_norm = 1e-05
highest = lax.Precision.HIGHEST

def causal_taps(history, current, weights):
    extended = jnp.concatenate([history, current], axis=0).astype(jnp.float32)
    length = current.shape[0]
    summed = extended[0:length] * weights[0].astype(jnp.float32)
    for offset in range(1, weights.shape[0]):
        summed = summed + extended[offset:offset + length] * weights[offset].astype(jnp.float32)
    return jax.nn.silu(summed)

def split_sum(left_rows, right_rows, pieces):
    slice_width = left_rows.shape[1] // pieces
    summed = jnp.zeros((left_rows.shape[0], right_rows.shape[1]), jnp.float32)
    for piece_index in range(pieces):
        low_col = piece_index * slice_width
        partial_sum = jnp.dot(left_rows[:, low_col:low_col + slice_width], right_rows[low_col:low_col + slice_width], preferred_element_type=jnp.float32)
        rounded = lax.optimization_barrier(partial_sum.astype(jnp.bfloat16))
        summed = summed + rounded.astype(jnp.float32)
    return summed

def reference(inner_pre, coeff_pre, gate_pre, step_raw, step_bias, decay_log, conv_inner, conv_coeff, mixer_gain, out_weight, residual, mlp_gain, up_weight, down_weight):
    per_group = INNER // HEAD_DIM // GROUPS
    blocks = SEQ // BLOCK
    edge_rows = CONV_TAPS - 1
    coeff_width = GROUPS * STATE
    decay_rate = jnp.exp(decay_log)
    position = jnp.arange(BLOCK)
    causal_mask = (position[:, None] >= position[None, :])[:, :, None, None]

    def one_block(running, inputs):
        ssm_state, inner_hist, coeff_hist = running
        inner_blk, coeff_blk, gate_blk, raw_blk, resid_blk = inputs
        inner_act = causal_taps(inner_hist, inner_blk, conv_inner)
        coeff_act = causal_taps(coeff_hist, coeff_blk, conv_coeff)
        in_coeff = coeff_act[:, 0].reshape(BLOCK, GROUPS, STATE)
        out_coeff = coeff_act[:, 1].reshape(BLOCK, GROUPS, STATE)
        step_size = jax.nn.softplus(raw_blk.astype(jnp.float32) + step_bias)
        log_step = (-step_size * decay_rate).reshape(BLOCK, GROUPS, per_group)
        values = inner_act.reshape(BLOCK, GROUPS, per_group, HEAD_DIM) * step_size.reshape(BLOCK, GROUPS, per_group)[..., None]
        log_cumul = jnp.cumsum(log_step, axis=0)
        log_gaps = log_cumul[:, None] - log_cumul[None, :]
        within = jnp.where(causal_mask, jnp.exp(jnp.where(causal_mask, log_gaps, 0.0)), 0.0)
        scores = jnp.einsum('lgn,sgn->lsg', out_coeff, in_coeff, precision=highest)
        inside = jnp.einsum('lsg,lsgh,sghp->lghp', scores, within, values, precision=highest)
        carried = jnp.einsum('lgn,ghpn,lgh->lghp', out_coeff, ssm_state, jnp.exp(log_cumul), precision=highest)
        to_end = jnp.exp(log_cumul[-1][None] - log_cumul)
        new_state = ssm_state * jnp.exp(log_cumul[-1])[..., None, None] + jnp.einsum('lgn,lgh,lghp->ghpn', in_coeff, to_end, values, precision=highest)
        gated = (inside + carried).reshape(BLOCK, INNER) * jax.nn.silu(gate_blk.astype(jnp.float32))
        grouped = gated.reshape(BLOCK, GROUPS, INNER // GROUPS)
        grouped = grouped * lax.rsqrt(lax.optimization_barrier(jnp.mean(grouped * grouped, axis=2, keepdims=True)) + eps_norm)
        mixed_rows = (grouped.reshape(BLOCK, INNER) * mixer_gain).astype(jnp.bfloat16)
        first_sum = (resid_blk.astype(jnp.float32) + split_sum(mixed_rows, out_weight, N_TP)).astype(jnp.bfloat16)
        first_wide = first_sum.astype(jnp.float32)
        normed = (first_wide * lax.rsqrt(lax.optimization_barrier(jnp.mean(first_wide * first_wide, axis=1, keepdims=True)) + eps_norm) * mlp_gain).astype(jnp.bfloat16)
        hidden = jnp.dot(normed, up_weight, preferred_element_type=jnp.float32)
        active = jnp.square(jax.nn.relu(hidden)).astype(jnp.bfloat16)
        result = (first_wide + split_sum(active, down_weight, N_TP)).astype(jnp.bfloat16)
        return ((new_state, inner_blk[BLOCK - edge_rows:], coeff_blk[BLOCK - edge_rows:]), result)
    start_state = jnp.zeros((GROUPS, per_group, HEAD_DIM, STATE), jnp.float32)
    start_inner = jnp.zeros((edge_rows, INNER), inner_pre.dtype)
    start_coeff = jnp.zeros((edge_rows, 2, coeff_width), coeff_pre.dtype)
    inputs = (inner_pre.reshape(blocks, BLOCK, INNER), coeff_pre.reshape(blocks, BLOCK, 2, coeff_width), gate_pre.reshape(blocks, BLOCK, INNER), step_raw.reshape(blocks, BLOCK, INNER // HEAD_DIM), residual.reshape(blocks, BLOCK, D))
    finals, outputs = lax.scan(one_block, (start_state, start_inner, start_coeff), inputs)
    return outputs.reshape(SEQ, D)
```

```python
import jax
import jax.numpy as jnp
from jax import lax
from jax.experimental import pallas as pl
from jax.experimental.pallas import tpu as pltpu
from jax.sharding import Mesh
from jax.sharding import PartitionSpec as P

MESH = pl.DeviceIdType.MESH
BF = jnp.bfloat16
F32 = jnp.float32
HIGH = lax.Precision.HIGHEST
EPS = 1e-05

ROWS = 384
HALF = ROWS // 2
BLOCK = 128
NB = ROWS // BLOCK
INNER = 512
STATE = 128
HEADS = 8
COLS = 256
FF = 1024
D = 2048
N = 8
NX = 4
PIECE = 32
SLICE = STATE // N
EDGE = 16


def dot(a, b, dims, precision=None):
    return lax.dot_general(a, b, (dims, ((), ())), precision=precision, preferred_element_type=F32)


NN = ((1,), (0,))
NT = ((1,), (1,))
TN = ((0,), (0,))


def per_head(v):
    low = lax.broadcasted_iota(jnp.int32, (v.shape[0], 128), 1) < 64
    tiles = [jnp.where(low, v[:, 2 * j : 2 * j + 1], v[:, 2 * j + 1 : 2 * j + 2]) for j in range(HEADS // 2)]
    return jnp.concatenate(tiles, axis=1)


def silu(v):
    return v / (1.0 + jnp.exp(-v))


def kernel(
    inner, coeff, gate, step_raw, step_bias, decay_log, taps_inner, taps_coeff, mixer_gain,
    out_hbm, residual, mlp_gain, up, down, result,
    hist_inner, hist_coeff, ext, act, cum, cum_t, step, step_t, local, states, own, enter,
    ld_own, ld_row, ld_total, ld_rows, pre, st_row, st_total, st_rows, st_back,
    mixed, out_w, up_all, down_all, gain_own, gain_all,
    pair_out, pair_in, far, relay_l, relay_r, near_l, near_r, keep_l, keep_r, fin_l, fin_r, keep,
    rows, first, acc, active,
    send, recv, w_send, w_recv, local_sem,
):
    z, y, x, c = (lax.axis_index(a) for a in ("z", "y", "x", "c"))
    tp = 2 * x + c
    at = lambda v, d: lax.rem(v + d, N)
    atx = lambda d: lax.rem(x + d, NX)
    next_id = {"z": at(z, jnp.where(y == N - 1, 1, 0)), "y": at(y, 1)}
    prev_id = {"z": at(z, jnp.where(y == 0, N - 1, 0)), "y": at(y, N - 1)}
    right, left = {"x": atx(1)}, {"x": atx(NX - 1)}
    partner = {"c": 1 - c}
    tp_id = lambda d: {"x": at(tp, d) // 2, "c": lax.rem(at(tp, d), 2)}

    barrier = pltpu.get_barrier_semaphore()
    greeted = [next_id, prev_id]
    for d in range(1, N):
        greeted += [{"y": at(y, d)}, {"z": at(z, d)}, tp_id(d)]
    for where in greeted:
        pl.semaphore_signal(barrier, inc=1, device_id=where, device_id_type=MESH)

    out_copy = pltpu.make_async_copy(out_hbm, out_w, local_sem)
    out_copy.start()

    started = []
    used = [0]

    def copy_to(src, dst, where, sems=None):
        if sems is None:
            sems = (send.at[used[0]], recv.at[used[0]])
            used[0] += 1
        copy = pltpu.make_async_remote_copy(
            src_ref=src, dst_ref=dst, send_sem=sems[0], recv_sem=sems[1], device_id=where, device_id_type=MESH
        )
        return copy

    def start(copy):
        copy.start()
        started.append(copy)
        return copy

    row_i = lax.broadcasted_iota(jnp.int32, (BLOCK, BLOCK), 0)
    col_i = lax.broadcasted_iota(jnp.int32, (BLOCK, BLOCK), 1)
    causal = row_i >= col_i
    tril = causal.astype(F32)
    triu = (row_i <= col_i).astype(F32)
    eye = (row_i == col_i).astype(F32)
    low_lanes = col_i < 64

    rate = jnp.exp(decay_log[...])
    ends = []
    for b in range(NB):
        rb = pl.ds(b * BLOCK, BLOCK)
        raw = step_raw[rb, :].astype(F32) + step_bias[...]
        size = jnp.maximum(raw, 0.0) + jnp.log1p(jnp.exp(-jnp.abs(raw)))
        logs = -size * rate
        cum_b = dot(tril, logs, NN, HIGH)
        cum[rb, :] = cum_b
        cum_t[:, rb] = dot(logs, triu, TN, HIGH)
        step[rb, :] = size
        step_t[:, rb] = dot(size, eye, TN, HIGH)
        ends.append(cum_b[BLOCK - 1 : BLOCK, :])
    total = ends[0] + ends[1] + ends[2]
    ld_own[...] = jnp.zeros_like(ld_own)
    ld_own[:, 0:HEADS] = jnp.broadcast_to(total, (8, HEADS))
    gain_own[...] = jnp.broadcast_to(mlp_gain[...], gain_own.shape)

    pl.semaphore_wait(barrier, len(greeted))

    tails = [
        start(copy_to(inner.at[pl.ds(ROWS - EDGE, EDGE)], hist_inner, next_id)),
        start(copy_to(coeff.at[pl.ds(ROWS - EDGE, EDGE)], hist_coeff, next_id)),
    ]
    ld_copies = [start(copy_to(ld_own, ld_row.at[y], {"y": at(y, d)})) for d in range(1, N)]
    gain_copies = [start(copy_to(gain_own, gain_all.at[tp], tp_id(d))) for d in range(1, N)]
    ld_row[y] = ld_own[...]
    gain_all[tp] = gain_own[...]

    first_up = [start(copy_to(up, up_all.at[z, y], {"z": at(z, d)})) for d in range(1, N)]
    first_down = [start(copy_to(down, down_all.at[z, y], {"y": at(y, d)})) for d in range(1, N)]
    up_all[z, y] = up[...]
    down_all[z, y] = down[...]

    def ring_copy(weight, way, hop, chunk):
        back = (N - (hop - 1)) % N if way == 0 else hop - 1
        part = pl.ds(4 * chunk, 4)
        if weight == 0:
            ref, where = up_all.at[part, at(y, back)], {"y": at(y, 1 if way == 0 else N - 1)}
        else:
            ref, where = down_all.at[at(z, back), part], {"z": at(z, 1 if way == 0 else N - 1)}
        i = ((weight * 2 + way) * 4 + hop - 1) * 2 + chunk
        return copy_to(ref, ref, where, (w_send.at[i], w_recv.at[i]))

    def ring_arrival(weight, way, hop, chunk):
        back = (N - hop) % N if way == 0 else hop
        part = pl.ds(4 * chunk, 4)
        if weight == 0:
            ref, where = up_all.at[part, at(y, back)], {"y": at(y, 1 if way == 0 else N - 1)}
        else:
            ref, where = down_all.at[at(z, back), part], {"z": at(z, 1 if way == 0 else N - 1)}
        i = ((weight * 2 + way) * 4 + hop - 1) * 2 + chunk
        copy_to(ref, ref, where, (w_send.at[i], w_recv.at[i])).wait_recv()

    def ring_first():
        for copy in first_up + first_down:
            copy.wait_recv()
        for chunk in range(2):
            for way in range(2):
                for weight in range(2):
                    start(ring_copy(weight, way, 1, chunk))

    def ring_next(hop, chunk):
        for way in range(2):
            for weight in range(2):
                ring_arrival(weight, way, hop - 1, chunk)
                start(ring_copy(weight, way, hop, chunk))

    def ring_last():
        for way in range(2):
            for weight in range(2):
                ring_arrival(weight, way, 3, way)
                start(ring_copy(weight, way, 4, way))

    def ring_end():
        for way in range(2):
            for weight in range(2):
                ring_arrival(weight, way, 3, 1 - way)
                ring_arrival(weight, way, 4, way)

    ext[8 : 8 + ROWS, 0:INNER] = inner[...].astype(F32)
    ext[8 : 8 + ROWS, INNER:] = coeff[...].astype(F32)

    def taps(b):
        for j in range(3):
            lanes = slice(COLS * j, COLS * (j + 1))
            weights = (taps_inner[:, lanes] if j < 2 else taps_coeff[...]).astype(F32)
            total_taps = ext[pl.ds(b * BLOCK + 5, BLOCK), lanes] * weights[0:1]
            for k in range(1, 4):
                total_taps = total_taps + ext[pl.ds(b * BLOCK + 5 + k, BLOCK), lanes] * weights[k : k + 1]
            act[b * BLOCK : (b + 1) * BLOCK, lanes] = silu(total_taps).astype(BF)

    def block_state(b):
        rb = slice(b * BLOCK, (b + 1) * BLOCK)
        weight = step[rb, :] * jnp.exp(ends[b] - cum[rb, :])
        values = act[rb, 0:INNER].astype(F32) * per_head(weight)
        states[b] = dot(act[rb, INNER : INNER + STATE], values.astype(BF), TN)

    taps(1)
    taps(2)
    block_state(1)
    block_state(2)
    for copy in tails:
        copy.wait_recv()
    is_first = jnp.logical_and(z == 0, y == 0)
    hist = jnp.concatenate([hist_inner[8:16, :].astype(F32), hist_coeff[8:16, :].astype(F32)], axis=1)
    ext[0:8, :] = jnp.where(is_first, 0.0, hist)
    taps(0)
    block_state(0)
    own[...] = (
        states[0] * per_head(jnp.exp(ends[1] + ends[2])) + states[1] * per_head(jnp.exp(ends[2])) + states[2]
    ).astype(BF)

    slice_of = lambda v: pl.ds(pl.multiple_of(v * SLICE, SLICE), SLICE)
    st1 = [start(copy_to(own.at[slice_of(at(y, d))], st_row.at[y], {"y": at(y, d)})) for d in range(1, N)]
    st_row[y] = own[slice_of(y), :]

    def inside(b):
        rb = slice(b * BLOCK, (b + 1) * BLOCK)
        scores = dot(act[rb, INNER + STATE :], act[rb, INNER : INNER + STATE], NT)
        for j in range(HEADS // 2):
            lanes = slice(128 * j, 128 * (j + 1))
            parts = []
            for h in (2 * j, 2 * j + 1):
                gap = cum[rb, h : h + 1] - cum_t[h : h + 1, rb]
                within = jnp.exp(jnp.where(causal, gap, -1e30)) * (scores * step_t[h : h + 1, rb])
                parts.append(dot(within.astype(BF), act[rb, lanes], NN))
            local[rb, lanes] = jnp.where(low_lanes, parts[0], parts[1])

    for copy in ld_copies:
        copy.wait_recv()
    row_logs = ld_row[:, 0, :]
    ld_total[...] = jnp.broadcast_to(jnp.sum(row_logs, axis=0, keepdims=True), (8, 128))
    ld2 = [start(copy_to(ld_total, ld_rows.at[z], {"z": at(z, d)})) for d in range(1, N)]
    ld_rows[z] = ld_total[...]
    row_decay = per_head(jnp.exp(row_logs))

    inside(0)
    for copy in st1:
        copy.wait_recv()
    run = jnp.zeros((SLICE, INNER), F32)
    for k in range(N):
        pre[k] = run
        run = run * row_decay[k : k + 1, :] + st_row[k].astype(F32)
    st_total[...] = run.astype(BF)
    st2 = [start(copy_to(st_total, st_rows.at[z], {"z": at(z, d)})) for d in range(1, N)]
    st_rows[z] = st_total[...]
    ring_first()
    inside(1)
    inside(2)
    for copy in ld2:
        copy.wait_recv()
    rows_decay = per_head(jnp.exp(ld_rows[:, 0, :]))
    for copy in st2:
        copy.wait_recv()
    run = jnp.zeros((SLICE, INNER), F32)
    for k in range(N):
        run = jnp.where(k < z, run * rows_decay[k : k + 1, :] + st_rows[k].astype(F32), run)
    for k in range(N):
        st_back[k] = (pre[k] + run).astype(BF)
        if k < N - 1:
            run = run * row_decay[k : k + 1, :]
    st3 = [
        start(copy_to(st_back.at[at(y, d)], enter.at[slice_of(y)], {"y": at(y, d)})) for d in range(1, N)
    ]
    enter[slice_of(y), :] = st_back[y]

    def carried(b):
        rb = slice(b * BLOCK, (b + 1) * BLOCK)
        if b == 1:
            inner_state = states[0]
        else:
            inner_state = states[0] * per_head(jnp.exp(ends[1])) + states[1]
        local[rb, :] += dot(act[rb, INNER + STATE :], inner_state.astype(BF), NN) * per_head(jnp.exp(cum[rb, :]))

    carried(1)
    carried(2)
    ring_next(2, 0)
    for copy in st3:
        copy.wait_recv()
    start_log = jnp.zeros_like(ends[0])
    for b in range(NB):
        rb = slice(b * BLOCK, (b + 1) * BLOCK)
        outer = dot(act[rb, INNER + STATE :], enter[...], NN) * per_head(jnp.exp(cum[rb, :] + start_log))
        gated = (local[rb, :] + outer) * silu(gate[rb, :].astype(F32))
        mean = jnp.mean(gated * gated, axis=1, keepdims=True)
        mixed[rb, :] = (gated * lax.rsqrt(mean + EPS) * mixer_gain[...]).astype(BF)
        start_log = start_log + ends[b]
    out_copy.wait()

    top, bottom = pl.ds(0, HALF), pl.ds(HALF, HALF)

    def reduced(block, use, pumps):
        pairs = []
        for i, dx in enumerate((2, 1, 3, 0)):
            pair_out[use, i] = block(2 * atx(dx) + 1 - c).astype(BF)
            pairs.append(start(copy_to(pair_out.at[use, i], pair_in.at[use, i], partner)))

        def mine(i, dx):
            value = block(2 * atx(dx) + c)
            pairs[i].wait_recv()
            return value + pair_in[use, i].astype(F32)

        far[use] = mine(0, 2).astype(BF)
        to_l = start(copy_to(far.at[use, top], relay_l.at[use], right))
        to_r = start(copy_to(far.at[use, bottom], relay_r.at[use], left))
        value = mine(1, 1)
        keep_r[...] = value[:HALF]
        near_r[use, HALF:, :] = value[HALF:].astype(BF)
        r_direct = start(copy_to(near_r.at[use, bottom], fin_l.at[use, bottom], right))
        value = mine(2, 3)
        keep_l[...] = value[HALF:]
        near_l[use, :HALF, :] = value[:HALF].astype(BF)
        l_direct = start(copy_to(near_l.at[use, top], fin_r.at[use, top], left))
        keep[...] = mine(3, 0)
        pumps[0]()
        to_l.wait_recv()
        near_r[use, :HALF, :] = (keep_r[...] + relay_l[use].astype(F32)).astype(BF)
        r_relay = start(copy_to(near_r.at[use, top], fin_l.at[use, top], right))
        to_r.wait_recv()
        near_l[use, HALF:, :] = (keep_l[...] + relay_r[use].astype(F32)).astype(BF)
        l_relay = start(copy_to(near_l.at[use, bottom], fin_r.at[use, bottom], left))
        pumps[1]()
        for copy in (r_direct, l_direct, r_relay, l_relay):
            copy.wait_recv()
        return keep[...] + fin_l[use].astype(F32) + fin_r[use].astype(F32)

    def out_block(owner):
        cols = pl.ds(pl.multiple_of(owner * COLS, COLS), COLS)
        return dot(mixed[...], out_w[:, cols], NN)

    projected = reduced(out_block, 0, (lambda: ring_next(2, 1), lambda: ring_next(3, 0)))
    first[...] = (residual[...].astype(F32) + projected).astype(BF)
    rows[tp] = first[...]

    mine_tp, left_tp, right_tp, far_tp = tp, 2 * atx(3) + c, 2 * atx(1) + c, 2 * atx(2) + c
    halves = {}
    halves["r0"] = start(copy_to(first.at[top], rows.at[tp, top], right))
    halves["l1"] = start(copy_to(first.at[bottom], rows.at[tp, bottom], left))
    across = [start(copy_to(first, rows.at[tp], partner))]
    halves["r1"] = start(copy_to(first.at[bottom], rows.at[tp, bottom], right))
    halves["l0"] = start(copy_to(first.at[top], rows.at[tp, top], left))
    for copy in gain_copies:
        copy.wait_recv()
    squares = jnp.zeros((ROWS, 1), F32)

    def raise_rows(source, squares, new=False):
        wide = rows[source].astype(F32)
        squares = squares + jnp.sum(wide * wide, axis=1, keepdims=True)
        scaled = (wide * gain_all[source][0:1, :]).astype(BF)
        weights = up_all[source].reshape(COLS, FF)
        product = dot(scaled, weights, NN)
        acc[...] = product if new else acc[...] + product
        return squares

    ring_next(3, 1)
    halves["r0"].wait_recv()
    fwd_r = start(copy_to(rows.at[left_tp, top], rows.at[left_tp, top], right))
    halves["l1"].wait_recv()
    fwd_l = start(copy_to(rows.at[right_tp, bottom], rows.at[right_tp, bottom], left))
    halves["r1"].wait_recv()
    across.append(start(copy_to(rows.at[left_tp], rows.at[left_tp], partner)))
    halves["l0"].wait_recv()
    across.append(start(copy_to(rows.at[right_tp], rows.at[right_tp], partner)))
    ring_last()
    fwd_r.wait_recv()
    fwd_l.wait_recv()
    across.append(start(copy_to(rows.at[far_tp], rows.at[far_tp], partner)))
    ring_end()
    squares = raise_rows(mine_tp, squares, True)
    squares = raise_rows(left_tp, squares)
    squares = raise_rows(right_tp, squares)
    squares = raise_rows(far_tp, squares)
    for copy, source in zip(across, (mine_tp, left_tp, right_tp, far_tp)):
        copy.wait_recv()
        squares = raise_rows(source + 1 - 2 * c, squares)
    scale = lax.rsqrt(squares * (1.0 / D) + EPS)
    active[...] = jnp.square(jnp.maximum(acc[...] * scale, 0.0)).astype(BF)

    def down_block(owner):
        return dot(active[...], down_all[owner].reshape(COLS, FF), NT)

    nothing = lambda: None
    lowered = reduced(down_block, 1, (nothing, nothing))
    result[...] = (first[...].astype(F32) + lowered).astype(BF)
    for copy in started:
        copy.wait_send()


def shards(
    inner_pre, coeff_pre, gate_pre, step_raw, step_bias, decay_log, conv_inner, conv_coeff, mixer_gain,
    out_weight, residual, mlp_gain, up_weight, down_weight,
):
    vm = pltpu.VMEM
    dma = pltpu.SemaphoreType.DMA
    in_vmem = pl.BlockSpec(memory_space=pltpu.VMEM)
    specs = [in_vmem] * 14
    specs[9] = pl.BlockSpec(memory_space=pl.ANY)
    scratch = [
        vm((EDGE, INNER), BF), vm((EDGE, COLS), BF), vm((ROWS + 8, INNER + COLS), F32), vm((ROWS, INNER + COLS), BF),
        vm((ROWS, HEADS), F32), vm((HEADS, ROWS), F32), vm((ROWS, HEADS), F32), vm((HEADS, ROWS), F32),
        vm((ROWS, INNER), F32), vm((NB, STATE, INNER), F32), vm((STATE, INNER), BF), vm((STATE, INNER), BF),
        vm((8, 128), F32), vm((N, 8, 128), F32), vm((8, 128), F32), vm((N, 8, 128), F32),
        vm((N, SLICE, INNER), F32), vm((N, SLICE, INNER), BF), vm((SLICE, INNER), BF), vm((N, SLICE, INNER), BF),
        vm((N, SLICE, INNER), BF),
        vm((ROWS, INNER), BF), vm((INNER, D), BF), vm((N, N, PIECE, FF), BF), vm((N, N, PIECE, FF), BF),
        vm((8, COLS), F32), vm((N, 8, COLS), F32),
        vm((2, NX, ROWS, COLS), BF), vm((2, NX, ROWS, COLS), BF), vm((2, ROWS, COLS), BF),
        vm((2, HALF, COLS), BF), vm((2, HALF, COLS), BF), vm((2, ROWS, COLS), BF), vm((2, ROWS, COLS), BF),
        vm((HALF, COLS), F32), vm((HALF, COLS), F32), vm((2, ROWS, COLS), BF), vm((2, ROWS, COLS), BF),
        vm((ROWS, COLS), F32),
        vm((N, ROWS, COLS), BF), vm((ROWS, COLS), BF), vm((ROWS, FF), F32), vm((ROWS, FF), BF),
        dma((96,)), dma((96,)), dma((32,)), dma((32,)), dma,
    ]
    return pl.pallas_call(
        kernel,
        out_shape=jax.ShapeDtypeStruct((ROWS, COLS), BF),
        in_specs=specs,
        out_specs=in_vmem,
        scratch_shapes=scratch,
        compiler_params=pltpu.CompilerParams(
            collective_id=0, has_side_effects=True, vmem_limit_bytes=60 * 1024 * 1024
        ),
        name="layer",
    )(
        inner_pre, coeff_pre.reshape(ROWS, COLS), gate_pre, step_raw, step_bias[None], decay_log[None], conv_inner,
        conv_coeff.reshape(4, COLS), mixer_gain[None], out_weight, residual, mlp_gain[None], up_weight, down_weight.T,
    )


def solution(mesh):
    split = Mesh(mesh.devices.reshape(N, N, NX, 2), ("z", "y", "x", "c"))
    sp, tp = ("z", "y"), ("x", "c")
    return jax.shard_map(
        shards,
        mesh=split,
        in_specs=(
            P(sp, tp), P(sp, None, tp), P(sp, tp), P(sp, tp), P(tp), P(tp), P(None, tp), P(None, None, tp), P(tp),
            P(tp, None), P(sp, tp), P(tp), P(sp, tp), P(tp, sp),
        ),
        out_specs=P(sp, tp),
        check_vma=False,
    )
```

```python
import jax
import jax.numpy as jnp
from jax import lax
from jax.experimental import pallas as pl
from jax.experimental.pallas import tpu as pltpu
from jax.sharding import Mesh
from jax.sharding import PartitionSpec as P

MESH = pl.DeviceIdType.MESH
BF = jnp.bfloat16
F32 = jnp.float32
HIGH = lax.Precision.HIGHEST
EPS = 1e-05

ROWS = 384
HALF = ROWS // 2
BLOCK = 128
NB = ROWS // BLOCK
INNER = 512
STATE = 128
HEADS = 8
COLS = 256
FF = 1024
D = 2048
N = 8
NX = 4
PIECE = 32
SLICE = STATE // N
EDGE = 16


def dot(a, b, dims, precision=None):
    return lax.dot_general(a, b, (dims, ((), ())), precision=precision, preferred_element_type=F32)


NN = ((1,), (0,))
NT = ((1,), (1,))
TN = ((0,), (0,))


def per_head(v):
    low = lax.broadcasted_iota(jnp.int32, (v.shape[0], 128), 1) < 64
    tiles = [jnp.where(low, v[:, 2 * j : 2 * j + 1], v[:, 2 * j + 1 : 2 * j + 2]) for j in range(HEADS // 2)]
    return jnp.concatenate(tiles, axis=1)


def silu(v):
    return v / (1.0 + jnp.exp(-v))


def kernel(
    inner_hbm, coeff_hbm, gate_hbm, step_raw, step_bias, decay_log, taps_inner, taps_coeff, mixer_gain,
    out_hbm, residual_hbm, mlp_gain, up_hbm, down_hbm, result,
    inner, coeff, gate, residual, up, down,
    hist_inner, hist_coeff, ext, ext_c, act, cum, cum_t, step, step_t, local, states, own, enter,
    ld_own, ld_row, ld_total, ld_rows, pre, st_row, st_total, st_rows, st_back,
    mixed, out_w, up_all, down_all, gain_own, gain_all,
    pair_out, pair_in, far, relay_l, relay_r, near_l, near_r, fin_l, fin_r, keep,
    rows, first, acc, active,
    send, recv, local_sem,
):
    z, y, x, c = (lax.axis_index(a) for a in ("z", "y", "x", "c"))
    tp = 2 * x + c
    at = lambda v, d: lax.rem(v + d, N)
    atx = lambda d: lax.rem(x + d, NX)
    next_id = {"z": at(z, jnp.where(y == N - 1, 1, 0)), "y": at(y, 1)}
    prev_id = {"z": at(z, jnp.where(y == 0, N - 1, 0)), "y": at(y, N - 1)}
    right, left = {"x": atx(1)}, {"x": atx(NX - 1)}
    partner = {"c": 1 - c}
    tp_id = lambda d: {"x": at(tp, d) // 2, "c": lax.rem(at(tp, d), 2)}

    barrier = pltpu.get_barrier_semaphore()
    greeted = [next_id, prev_id]
    for d in range(1, N):
        greeted += [{"y": at(y, d)}, {"z": at(z, d)}, tp_id(d)]
    for where in greeted:
        pl.semaphore_signal(barrier, inc=1, device_id=where, device_id_type=MESH)

    fetched = [
        pltpu.make_async_copy(there, here, local_sem.at[i])
        for i, (there, here) in enumerate(
            (
                (up_hbm, up), (down_hbm, down), (inner_hbm, inner), (coeff_hbm, coeff), (gate_hbm, gate),
                (residual_hbm, residual), (out_hbm, out_w),
            )
        )
    ]
    for copy in fetched:
        copy.start()
    up_copy, down_copy, inner_copy, coeff_copy, gate_copy, residual_copy, out_copy = fetched

    used = [0, 0]
    pending = []

    def remote(src, dst, where, sent, arrived):
        return pltpu.make_async_remote_copy(
            src_ref=src, dst_ref=dst, send_sem=sent, recv_sem=arrived, device_id=where, device_id_type=MESH
        )

    def sender(total):
        used[0] += 1
        pending.append((send.at[used[0] - 1], total))
        return send.at[used[0] - 1]

    def receiver():
        used[1] += 1
        return recv.at[used[1] - 1]

    def go(*args):
        remote(*args).start()

    def landed(arrived, total):
        remote(total, total, partner, send.at[0], arrived).wait_recv()

    row_i = lax.broadcasted_iota(jnp.int32, (BLOCK, BLOCK), 0)
    col_i = lax.broadcasted_iota(jnp.int32, (BLOCK, BLOCK), 1)
    causal = row_i >= col_i
    tril = causal.astype(F32)
    triu = (row_i <= col_i).astype(F32)
    eye = (row_i == col_i).astype(F32)
    low_lanes = col_i < 64

    on_heads = lax.broadcasted_iota(jnp.int32, (HEADS, HEADS), 0) == lax.broadcasted_iota(jnp.int32, (HEADS, HEADS), 1)
    column = lambda v: jnp.sum(jnp.where(on_heads, jnp.broadcast_to(v, (HEADS, HEADS)), 0.0), axis=1, keepdims=True)
    bias = column(step_bias[...])
    rate = jnp.exp(column(decay_log[...]))
    ends = []
    for b in range(NB):
        rb = pl.ds(b * BLOCK, BLOCK)
        raw = step_raw[:, rb].astype(F32) + bias
        size = jnp.maximum(raw, 0.0) + jnp.log1p(jnp.exp(-jnp.abs(raw)))
        logs = -size * rate
        cum_b = dot(tril, logs, NT, HIGH)
        cum[rb, :] = cum_b
        cum_t[:, rb] = dot(logs, triu, NN, HIGH)
        step[rb, :] = dot(eye, size, NT, HIGH)
        step_t[:, rb] = size
        ends.append(cum_b[BLOCK - 1 : BLOCK, :])
    total = ends[0] + ends[1] + ends[2]
    ld_own[...] = jnp.zeros_like(ld_own)
    ld_own[:, 0:HEADS] = jnp.broadcast_to(total, (8, HEADS))
    gain_own[...] = jnp.broadcast_to(mlp_gain[...], gain_own.shape)

    pl.semaphore_wait(barrier, len(greeted))

    inner_copy.wait()
    coeff_copy.wait()
    inner_tail, coeff_tail = receiver(), receiver()
    go(inner.at[pl.ds(ROWS - EDGE, EDGE)], hist_inner, next_id, sender(hist_inner), inner_tail)
    go(coeff.at[pl.ds(ROWS - 8, 8)], hist_coeff, next_id, sender(hist_coeff), coeff_tail)
    seven = pl.ds(0, N - 1)

    def to_all(source, target, where):
        sent, arrived = sender(target[1]), receiver()
        for d in range(1, N):
            go(source(d), target[0], where(d), sent, arrived)
        return lambda: landed(arrived, target[1])

    along_y, along_z = lambda d: {"y": at(y, d)}, lambda d: {"z": at(z, d)}
    ld_landed = to_all(lambda d: ld_own, (ld_row.at[y], ld_row.at[seven]), along_y)
    gain_landed = to_all(lambda d: gain_own, (gain_all.at[tp], gain_all.at[seven]), tp_id)
    ld_row[y] = ld_own[...]
    gain_all[tp] = gain_own[...]

    up_copy.wait()
    down_copy.wait()
    OFFSETS = ((0,), (N - 1, 1), (N - 2, 2), (N - 3, 3), (4,))
    weights_sent = [[sender(w.at[0, seven]), sender(w.at[seven])] for w in (up_all, down_all)]
    weights_landed = [
        [[receiver() for _ in range(4)], [[receiver() for _ in range(5)] for _ in range(4)]] for _ in range(2)
    ]

    def forward(weight, stage, way, hop, batch=0, offset=0):
        back = (N - (hop - 1)) % N if way == 0 else hop - 1
        to = 1 if way == 0 else N - 1
        a, b = (z, y) if weight == 0 else (y, z)
        a_axis, b_axis = ("z", "y") if weight == 0 else ("y", "z")
        arrived = weights_landed[weight][stage][hop - 1]
        if stage == 0:
            ia, ib, where = at(a, back), b, {a_axis: at(a, to)}
        else:
            ia, ib, where = at(a, offset), at(b, back), {b_axis: at(b, to)}
            arrived = arrived[batch]
        ref = up_all.at[ia, ib] if weight == 0 else down_all.at[ib, ia]
        source = ref
        if hop == 1 and offset == 0:
            source = up if weight == 0 else down
        if hop == 4:
            ref = source = ref.at[pl.ds(16 * way, 16)]
        go(source, ref, where, weights_sent[weight][stage], arrived)

    def pieces_landed(weight, stage, hop, batch=0):
        count = len(OFFSETS[batch]) * (1 if hop == 4 else 2)
        arrived = weights_landed[weight][stage][hop - 1]
        if stage == 0:
            arrived, count = arrived, 1 if hop == 4 else 2
        else:
            arrived = arrived[batch]
        landed(arrived, (up_all if weight == 0 else down_all).at[0, pl.ds(0, count)])

    def along(hop):
        for w in range(2):
            if hop > 1:
                pieces_landed(w, 0, hop - 1)
            if hop < 5:
                forward(w, 0, 0, hop)
                forward(w, 0, 1, hop)

    def across_to(hop, batch):
        for w in range(2):
            if hop > 1:
                pieces_landed(w, 1, hop - 1, batch)
            for offset in OFFSETS[batch]:
                forward(w, 1, 0, hop, batch, offset)
                forward(w, 1, 1, hop, batch, offset)

    def event(k):
        if k < 5:
            along(k + 1)
        for hop, batch in EVENTS[k]:
            across_to(hop, batch)

    EVENTS = (
        ((1, 0),),
        ((1, 1),),
        ((1, 2), (2, 0)),
        ((1, 3), (2, 1)),
        ((1, 4), (2, 2), (3, 0)),
        ((2, 3), (3, 1)),
        ((2, 4), (3, 2), (4, 0)),
        ((3, 3), (4, 1)),
        ((3, 4), (4, 2)),
        ((4, 3),),
        ((4, 4),),
    )
    event(0)
    up_all[z, y] = up[...]
    down_all[z, y] = down[...]

    ext[8 : 8 + ROWS, :] = inner[...].astype(F32)
    ext_c[8 : 8 + ROWS] = coeff[...].astype(F32)

    def taps(b):
        for j in range(4):
            if j < 2:
                lanes = slice(COLS * j, COLS * (j + 1))
                weights = taps_inner[:, lanes].astype(F32)
                shifted = lambda k: ext[pl.ds(b * BLOCK + 5 + k, BLOCK), lanes]
                target = lanes
            else:
                weights = taps_coeff[...].astype(F32)[:, j - 2, :]
                shifted = lambda k: ext_c[pl.ds(b * BLOCK + 5 + k, BLOCK), j - 2, :]
                target = slice(INNER + STATE * (j - 2), INNER + STATE * (j - 1))
            total_taps = shifted(0) * weights[0:1]
            for k in range(1, 4):
                total_taps = total_taps + shifted(k) * weights[k : k + 1]
            act[b * BLOCK : (b + 1) * BLOCK, target] = silu(total_taps).astype(BF)

    def block_state(b):
        rb = slice(b * BLOCK, (b + 1) * BLOCK)
        weight = step[rb, :] * jnp.exp(ends[b] - cum[rb, :])
        values = act[rb, 0:INNER].astype(F32) * per_head(weight)
        states[b] = dot(act[rb, INNER : INNER + STATE], values.astype(BF), TN)

    taps(1)
    taps(2)
    block_state(1)
    block_state(2)
    landed(inner_tail, hist_inner)
    landed(coeff_tail, hist_coeff)
    is_first = jnp.logical_and(z == 0, y == 0)
    ext[0:8, :] = jnp.where(is_first, 0.0, hist_inner[8:16, :].astype(F32))
    ext_c[0:8] = jnp.where(is_first, 0.0, hist_coeff[...].astype(F32))
    taps(0)
    block_state(0)
    own[...] = (
        states[0] * per_head(jnp.exp(ends[1] + ends[2])) + states[1] * per_head(jnp.exp(ends[2])) + states[2]
    ).astype(BF)

    slice_of = lambda v: pl.ds(pl.multiple_of(v * SLICE, SLICE), SLICE)
    st1_landed = to_all(lambda d: own.at[slice_of(at(y, d))], (st_row.at[y], st_row.at[seven]), along_y)
    event(1)
    st_row[y] = own[slice_of(y), :]

    def inside(b):
        rb = slice(b * BLOCK, (b + 1) * BLOCK)
        scores = dot(act[rb, INNER + STATE :], act[rb, INNER : INNER + STATE], NT)
        for j in range(HEADS // 2):
            lanes = slice(128 * j, 128 * (j + 1))
            parts = []
            for h in (2 * j, 2 * j + 1):
                gap = cum[rb, h : h + 1] - cum_t[h : h + 1, rb]
                within = jnp.exp(jnp.where(causal, gap, -1e30)) * (scores * step_t[h : h + 1, rb])
                parts.append(dot(within.astype(BF), act[rb, lanes], NN))
            local[rb, lanes] = jnp.where(low_lanes, parts[0], parts[1])

    def carried(b):
        rb = slice(b * BLOCK, (b + 1) * BLOCK)
        if b == 1:
            inner_state = states[0]
        else:
            inner_state = states[0] * per_head(jnp.exp(ends[1])) + states[1]
        local[rb, :] += dot(act[rb, INNER + STATE :], inner_state.astype(BF), NN) * per_head(jnp.exp(cum[rb, :]))

    ld_landed()
    row_logs = ld_row[:, 0, :]
    ld_total[...] = jnp.broadcast_to(jnp.sum(row_logs, axis=0, keepdims=True), (8, 128))
    ld2_landed = to_all(lambda d: ld_total, (ld_rows.at[z], ld_rows.at[seven]), along_z)
    ld_rows[z] = ld_total[...]
    row_decay = per_head(jnp.exp(row_logs))

    inside(0)
    inside(1)
    inside(2)
    carried(1)
    carried(2)
    st1_landed()
    run = jnp.zeros((SLICE, INNER), F32)
    for k in range(N):
        pre[k] = run
        run = run * row_decay[k : k + 1, :] + st_row[k].astype(F32)
    st_total[...] = run.astype(BF)
    st2_landed = to_all(lambda d: st_total, (st_rows.at[z], st_rows.at[seven]), along_z)
    st_rows[z] = st_total[...]
    event(2)
    ld2_landed()
    rows_decay = per_head(jnp.exp(ld_rows[:, 0, :]))
    st2_landed()
    run = jnp.zeros((SLICE, INNER), F32)
    for k in range(N):
        run = jnp.where(k < z, run * rows_decay[k : k + 1, :] + st_rows[k].astype(F32), run)
    for k in range(N):
        st_back[k] = (pre[k] + run).astype(BF)
        if k < N - 1:
            run = run * row_decay[k : k + 1, :]
    st3_landed = to_all(
        lambda d: st_back.at[at(y, d)], (enter.at[slice_of(y)], enter.at[pl.ds(0, SLICE * (N - 1))]), along_y
    )
    enter[slice_of(y), :] = st_back[y]

    event(3)
    st3_landed()
    event(4)
    gate_copy.wait()
    start_log = jnp.zeros_like(ends[0])
    for b in range(NB):
        rb = slice(b * BLOCK, (b + 1) * BLOCK)
        outer = dot(act[rb, INNER + STATE :], enter[...], NN) * per_head(jnp.exp(cum[rb, :] + start_log))
        gated = (local[rb, :] + outer) * silu(gate[rb, :].astype(F32))
        mean = jnp.mean(gated * gated, axis=1, keepdims=True)
        mixed[rb, :] = (gated * lax.rsqrt(mean + EPS) * mixer_gain[...]).astype(BF)
        start_log = start_log + ends[b]

    top, bottom = pl.ds(0, HALF), pl.ds(HALF, HALF)

    def reduced(block, use, pumps):
        pair_sent, ring_sent = sender(rows.at[pl.ds(0, NX)]), sender(rows.at[pl.ds(0, 3)])
        pair_landed = [receiver() for _ in range(NX)]
        from_l, from_r, final = receiver(), receiver(), receiver()

        def both(i, dx):
            value = block(atx(dx))
            lower, upper = value[:, :COLS], value[:, COLS:]
            pair_out[use, i] = jnp.where(c == 0, upper, lower).astype(BF)
            go(pair_out.at[use, i], pair_in.at[use, i], partner, pair_sent, pair_landed[i])
            keep[i] = jnp.where(c == 0, lower, upper)

        def mine(i):
            landed(pair_landed[i], rows.at[0])
            return keep[i] + pair_in[use, i].astype(F32)

        both(0, 2)
        both(1, 1)
        pumps[0]()
        far[use] = mine(0).astype(BF)
        go(far.at[use, top], relay_l.at[use], right, ring_sent, from_l)
        go(far.at[use, bottom], relay_r.at[use], left, ring_sent, from_r)
        both(2, 3)
        value = mine(1)
        keep[1] = value
        near_r[use, HALF:, :] = value[HALF:].astype(BF)
        go(near_r.at[use, bottom], fin_l.at[use, bottom], right, ring_sent, final)
        both(3, 0)
        value = mine(2)
        keep[2] = value
        near_l[use, :HALF, :] = value[:HALF].astype(BF)
        go(near_l.at[use, top], fin_r.at[use, top], left, ring_sent, final)
        keep[3] = mine(3)
        landed(from_l, relay_l.at[use])
        near_r[use, :HALF, :] = (keep[1, :HALF, :] + relay_l[use].astype(F32)).astype(BF)
        go(near_r.at[use, top], fin_l.at[use, top], right, ring_sent, final)
        landed(from_r, relay_r.at[use])
        near_l[use, HALF:, :] = (keep[2, HALF:, :] + relay_r[use].astype(F32)).astype(BF)
        go(near_l.at[use, bottom], fin_r.at[use, bottom], left, ring_sent, final)
        pumps[1]()
        landed(final, rows.at[pl.ds(0, 2)])
        return keep[3] + fin_l[use].astype(F32) + fin_r[use].astype(F32)

    def out_block(chip):
        return dot(mixed[...], out_w[:, pl.ds(pl.multiple_of(chip * 2 * COLS, 2 * COLS), 2 * COLS)], NN)

    out_copy.wait()
    projected = reduced(out_block, 0, (lambda: event(5), lambda: event(6)))
    residual_copy.wait()
    first[...] = (residual[...].astype(F32) + projected).astype(BF)
    rows[tp] = first[...]

    mine_tp, left_tp, right_tp, far_tp = tp, 2 * atx(3) + c, 2 * atx(1) + c, 2 * atx(2) + c
    rows_sent = sender(rows.at[seven])
    l_first, r_first, l_second, r_second, far_landed, across_landed = (receiver() for _ in range(6))
    go(first.at[top], rows.at[tp, top], right, rows_sent, l_first)
    go(first.at[bottom], rows.at[tp, bottom], left, rows_sent, r_first)
    go(first, rows.at[tp], partner, rows_sent, across_landed)
    go(first.at[bottom], rows.at[tp, bottom], right, rows_sent, l_second)
    go(first.at[top], rows.at[tp, top], left, rows_sent, r_second)
    event(7)
    gain_landed()
    squares = jnp.zeros((ROWS, 1), F32)

    def raise_rows(source, squares, new=False):
        wide = rows[source].astype(F32)
        squares = squares + jnp.sum(wide * wide, axis=1, keepdims=True)
        scaled = (wide * gain_all[source][0:1, :]).astype(BF)
        weights = up_all[source].reshape(COLS, FF)
        product = dot(scaled, weights, NN)
        acc[...] = product if new else acc[...] + product
        return squares

    landed(l_first, relay_l.at[0])
    go(rows.at[left_tp, top], rows.at[left_tp, top], right, rows_sent, far_landed)
    landed(r_first, relay_l.at[0])
    go(rows.at[right_tp, bottom], rows.at[right_tp, bottom], left, rows_sent, far_landed)
    landed(l_second, relay_l.at[0])
    go(rows.at[left_tp], rows.at[left_tp], partner, rows_sent, across_landed)
    landed(r_second, relay_l.at[0])
    go(rows.at[right_tp], rows.at[right_tp], partner, rows_sent, across_landed)
    event(8)
    landed(far_landed, rows.at[0])
    go(rows.at[far_tp], rows.at[far_tp], partner, rows_sent, across_landed)
    landed(across_landed, rows.at[pl.ds(0, NX)])
    event(9)
    for batch in range(2):
        pieces_landed(0, 1, 4, batch)
    for k in (0, N - 1, 1):
        squares = raise_rows(at(z, k), squares, k == 0)
    event(10)
    for batch, sources in ((2, (N - 2, 2)), (3, (N - 3, 3)), (4, (4,))):
        pieces_landed(0, 1, 4, batch)
        for k in sources:
            squares = raise_rows(at(z, k), squares)
    scale = lax.rsqrt(squares * (1.0 / D) + EPS)
    active[...] = jnp.square(jnp.maximum(acc[...] * scale, 0.0)).astype(BF)

    def down_block(chip):
        return dot(active[...], down_all[pl.ds(2 * chip, 2)].reshape(2 * COLS, FF), NT)

    for batch in range(5):
        pieces_landed(1, 1, 4, batch)
    nothing = lambda: None
    lowered = reduced(down_block, 1, (nothing, nothing))
    result[...] = (first[...].astype(F32) + lowered).astype(BF)
    for sent, total in pending:
        remote(total, total, partner, sent, recv.at[0]).wait_send()


def shards(
    inner_pre, coeff_pre, gate_pre, step_raw, step_bias, decay_log, conv_inner, conv_coeff, mixer_gain,
    out_weight, residual, mlp_gain, up_weight, down_weight,
):
    vm = pltpu.VMEM
    dma = pltpu.SemaphoreType.DMA
    in_vmem = pl.BlockSpec(memory_space=pltpu.VMEM)
    specs = [in_vmem] * 14
    for i in (0, 1, 2, 9, 10, 12, 13):
        specs[i] = pl.BlockSpec(memory_space=pl.ANY)
    scratch = [
        vm((ROWS, INNER), BF), vm((ROWS, 2, STATE), BF), vm((ROWS, INNER), BF), vm((ROWS, COLS), BF),
        vm((PIECE, FF), BF), vm((PIECE, FF), BF),
        vm((EDGE, INNER), BF), vm((8, 2, STATE), BF), vm((ROWS + 8, INNER), F32), vm((ROWS + 8, 2, STATE), F32), vm((ROWS, INNER + COLS), BF),
        vm((ROWS, HEADS), F32), vm((HEADS, ROWS), F32), vm((ROWS, HEADS), F32), vm((HEADS, ROWS), F32),
        vm((ROWS, INNER), F32), vm((NB, STATE, INNER), F32), vm((STATE, INNER), BF), vm((STATE, INNER), BF),
        vm((8, 128), F32), vm((N, 8, 128), F32), vm((8, 128), F32), vm((N, 8, 128), F32),
        vm((N, SLICE, INNER), F32), vm((N, SLICE, INNER), BF), vm((SLICE, INNER), BF), vm((N, SLICE, INNER), BF),
        vm((N, SLICE, INNER), BF),
        vm((ROWS, INNER), BF), vm((INNER, D), BF), vm((N, N, PIECE, FF), BF), vm((N, N, PIECE, FF), BF),
        vm((8, COLS), F32), vm((N, 8, COLS), F32),
        vm((2, NX, ROWS, COLS), BF), vm((2, NX, ROWS, COLS), BF), vm((2, ROWS, COLS), BF),
        vm((2, HALF, COLS), BF), vm((2, HALF, COLS), BF), vm((2, ROWS, COLS), BF), vm((2, ROWS, COLS), BF),
        vm((2, ROWS, COLS), BF), vm((2, ROWS, COLS), BF), vm((NX, ROWS, COLS), F32),
        vm((N, ROWS, COLS), BF), vm((ROWS, COLS), BF), vm((ROWS, FF), F32), vm((ROWS, FF), BF),
        dma((17,)), dma((76,)), dma((7,)),
    ]
    return pl.pallas_call(
        kernel,
        out_shape=jax.ShapeDtypeStruct((ROWS, COLS), BF),
        in_specs=specs,
        out_specs=in_vmem,
        scratch_shapes=scratch,
        compiler_params=pltpu.CompilerParams(
            collective_id=0, has_side_effects=True, vmem_limit_bytes=60 * 1024 * 1024
        ),
        name="layer",
    )(
        inner_pre, coeff_pre, gate_pre, step_raw.T, step_bias[None], decay_log[None], conv_inner,
        conv_coeff, mixer_gain[None], out_weight, residual, mlp_gain[None], up_weight, down_weight.T,
    )


def solution(mesh):
    split = Mesh(mesh.devices.reshape(N, N, NX, 2), ("z", "y", "x", "c"))
    sp, tp = ("z", "y"), ("x", "c")
    return jax.shard_map(
        shards,
        mesh=split,
        in_specs=(
            P(sp, tp), P(sp, None, tp), P(sp, tp), P(sp, tp), P(tp), P(tp), P(None, tp), P(None, None, tp), P(tp),
            P(tp, None), P(sp, tp), P(tp), P(sp, tp), P(tp, sp),
        ),
        out_specs=P(sp, tp),
        check_vma=False,
    )
```

```python
import jax
import jax.numpy as jnp
from jax import lax
from jax.experimental import pallas as pl
from jax.experimental.pallas import tpu as pltpu
from jax.sharding import Mesh
from jax.sharding import PartitionSpec as P

MESH = pl.DeviceIdType.MESH
BF = jnp.bfloat16
F32 = jnp.float32
HIGH = lax.Precision.HIGHEST
EPS = 1e-05

ROWS = 384
HALF = ROWS // 2
BLOCK = 128
NB = ROWS // BLOCK
INNER = 512
STATE = 128
HEADS = 8
COLS = 256
FF = 1024
D = 2048
N = 8
NX = 4
PIECE = 32
SLICE = STATE // N
EDGE = 16


def dot(a, b, dims, precision=None):
    return lax.dot_general(a, b, (dims, ((), ())), precision=precision, preferred_element_type=F32)


NN = ((1,), (0,))
NT = ((1,), (1,))
TN = ((0,), (0,))


def per_head(v):
    low = lax.broadcasted_iota(jnp.int32, (v.shape[0], 128), 1) < 64
    tiles = [jnp.where(low, v[:, 2 * j : 2 * j + 1], v[:, 2 * j + 1 : 2 * j + 2]) for j in range(HEADS // 2)]
    return jnp.concatenate(tiles, axis=1)


def silu(v):
    return v / (1.0 + jnp.exp(-v))


def kernel(
    inner_hbm, coeff_hbm, gate_hbm, step_raw_hbm, step_bias_hbm, decay_log_hbm, taps_inner_hbm, taps_coeff_hbm,
    mixer_gain_hbm, out_hbm, residual_hbm, mlp_gain_hbm, up_hbm, down_hbm, result,
    inner, coeff, gate, residual, up, down, step_raw, step_bias, decay_log, taps_inner, taps_coeff, mixer_gain,
    mlp_gain,
    hist_inner, hist_coeff, ext, ext_c, act, cum, cum_t, step, step_t, local, states, own, enter,
    ld_own, ld_row, ld_total, ld_rows, pre, st_row, st_total, st_rows, st_back,
    mixed, out_w, up_all, down_all, gain_own, gain_all,
    rows, first, acc, active, send, recv, local_sem, *reductions,
):
    z, y, x, c = (lax.axis_index(a) for a in ("z", "y", "x", "c"))
    tp = 2 * x + c
    at = lambda v, d: lax.rem(v + d, N)
    atx = lambda d: lax.rem(x + d, NX)
    next_id = {"z": at(z, jnp.where(y == N - 1, 1, 0)), "y": at(y, 1)}
    prev_id = {"z": at(z, jnp.where(y == 0, N - 1, 0)), "y": at(y, N - 1)}
    right, left = {"x": atx(1)}, {"x": atx(NX - 1)}
    partner = {"c": 1 - c}
    tp_id = lambda d: {"x": at(tp, d) // 2, "c": lax.rem(at(tp, d), 2)}

    barrier = pltpu.get_barrier_semaphore()
    greeted = [next_id, prev_id]
    for d in range(1, N):
        greeted += [{"y": at(y, d)}, {"z": at(z, d)}, tp_id(d)]
    for where in greeted:
        pl.semaphore_signal(barrier, inc=1, device_id=where, device_id_type=MESH)

    fetched = [
        pltpu.make_async_copy(there, here, local_sem.at[i])
        for i, (there, here) in enumerate(
            (
                (step_raw_hbm, step_raw), (step_bias_hbm, step_bias), (decay_log_hbm, decay_log),
                (mlp_gain_hbm, mlp_gain), (taps_inner_hbm, taps_inner), (taps_coeff_hbm, taps_coeff),
                (up_hbm, up), (down_hbm, down), (inner_hbm, inner), (coeff_hbm, coeff),
                (mixer_gain_hbm, mixer_gain), (gate_hbm, gate), (residual_hbm, residual), (out_hbm, out_w),
            )
        )
    ]
    for copy in fetched:
        copy.start()
    up_copy, down_copy, inner_copy, coeff_copy, mixer_gain_copy, gate_copy, residual_copy, out_copy = fetched[6:]

    used = [0, 0]
    pending = []

    def remote(src, dst, where, sent, arrived):
        return pltpu.make_async_remote_copy(
            src_ref=src, dst_ref=dst, send_sem=sent, recv_sem=arrived, device_id=where, device_id_type=MESH
        )

    def sender(total):
        used[0] += 1
        pending.append((send.at[used[0] - 1], total))
        return send.at[used[0] - 1]

    def receiver():
        used[1] += 1
        return recv.at[used[1] - 1]

    def go(*args):
        remote(*args).start()

    def landed(arrived, total):
        remote(total, total, partner, send.at[0], arrived).wait_recv()

    row_i = lax.broadcasted_iota(jnp.int32, (BLOCK, BLOCK), 0)
    col_i = lax.broadcasted_iota(jnp.int32, (BLOCK, BLOCK), 1)
    causal = row_i >= col_i
    tril = causal.astype(F32)
    triu = (row_i <= col_i).astype(F32)
    eye = (row_i == col_i).astype(F32)
    low_lanes = col_i < 64

    on_heads = lax.broadcasted_iota(jnp.int32, (HEADS, HEADS), 0) == lax.broadcasted_iota(jnp.int32, (HEADS, HEADS), 1)
    column = lambda v: jnp.sum(jnp.where(on_heads, jnp.broadcast_to(v, (HEADS, HEADS)), 0.0), axis=1, keepdims=True)
    for copy in fetched[:6]:
        copy.wait()
    bias = column(step_bias[...])
    rate = jnp.exp(column(decay_log[...]))
    ends = []
    for b in range(NB):
        rb = pl.ds(b * BLOCK, BLOCK)
        raw = step_raw[:, rb].astype(F32) + bias
        size = jnp.maximum(raw, 0.0) + jnp.log1p(jnp.exp(-jnp.abs(raw)))
        logs = -size * rate
        cum_b = dot(tril, logs, NT, HIGH)
        cum[rb, :] = cum_b
        cum_t[:, rb] = dot(logs, triu, NN, HIGH)
        step[rb, :] = dot(eye, size, NT, HIGH)
        step_t[:, rb] = size
        ends.append(cum_b[BLOCK - 1 : BLOCK, :])
    total = ends[0] + ends[1] + ends[2]
    ld_own[...] = jnp.zeros_like(ld_own)
    ld_own[:, 0:HEADS] = jnp.broadcast_to(total, (8, HEADS))
    gain_own[...] = jnp.broadcast_to(mlp_gain[...], gain_own.shape)

    pl.semaphore_wait(barrier, len(greeted))

    inner_copy.wait()
    coeff_copy.wait()
    inner_tail, coeff_tail = receiver(), receiver()
    go(inner.at[pl.ds(ROWS - EDGE, EDGE)], hist_inner, next_id, sender(hist_inner), inner_tail)
    go(coeff.at[pl.ds(ROWS - 8, 8)], hist_coeff, next_id, sender(hist_coeff), coeff_tail)
    seven = pl.ds(0, N - 1)

    def to_all(source, target, where):
        sent, arrived = sender(target[1]), receiver()
        for d in range(1, N):
            go(source(d), target[0], where(d), sent, arrived)
        return lambda: landed(arrived, target[1])

    along_y, along_z = lambda d: {"y": at(y, d)}, lambda d: {"z": at(z, d)}
    ld_landed = to_all(lambda d: ld_own, (ld_row.at[y], ld_row.at[seven]), along_y)
    gain_landed = to_all(lambda d: gain_own, (gain_all.at[tp], gain_all.at[seven]), tp_id)
    ld_row[y] = ld_own[...]
    gain_all[tp] = gain_own[...]

    up_copy.wait()
    down_copy.wait()
    OFFSETS = ((0,), (N - 1, 1), (N - 2, 2), (N - 3, 3), (4,))
    weights_sent = [[sender(w.at[0, seven]), sender(w.at[seven])] for w in (up_all, down_all)]
    weights_landed = [
        [[receiver() for _ in range(4)], [[receiver() for _ in range(5)] for _ in range(4)]] for _ in range(2)
    ]

    def forward(weight, stage, way, hop, batch=0, offset=0):
        back = (N - (hop - 1)) % N if way == 0 else hop - 1
        to = 1 if way == 0 else N - 1
        whole, piece = (up_all, up) if weight == 0 else (down_all, down)
        arrived = weights_landed[weight][stage][hop - 1]
        arrived = arrived if stage == 0 else arrived[batch]
        columns = slice(None) if hop < 4 else pl.ds(way * (FF // 2), FF // 2)
        for order in range(2):
            part = pl.ds(order * (PIECE // 2), PIECE // 2)
            a, b = (z, y) if order == 0 else (y, z)
            if stage == 0:
                ia, ib = at(a, back), b
            else:
                ia, ib = at(a, offset), at(b, back)
            on_z = (stage == 0) == (order == 0)
            where = {"z": at(z, to)} if on_z else {"y": at(y, to)}
            iz, iy = (ia, ib) if order == 0 else (ib, ia)
            ref = whole.at[iz, iy, part, columns]
            source = piece.at[part] if hop == 1 and offset == 0 else ref
            go(source, ref, where, weights_sent[weight][stage], arrived)

    def pieces_landed(weight, stage, hop, batch=0):
        count = len(OFFSETS[batch]) * (1 if hop == 4 else 2)
        arrived = weights_landed[weight][stage][hop - 1]
        if stage == 0:
            arrived, count = arrived, 1 if hop == 4 else 2
        else:
            arrived = arrived[batch]
        landed(arrived, (up_all if weight == 0 else down_all).at[0, pl.ds(0, count)])

    def along(weight, hop):
        if hop > 1:
            pieces_landed(weight, 0, hop - 1)
        if hop < 5:
            forward(weight, 0, 0, hop)
            forward(weight, 0, 1, hop)

    def across_to(weight, hop, batch):
        if hop > 1:
            pieces_landed(weight, 1, hop - 1, batch)
        for offset in OFFSETS[batch]:
            forward(weight, 1, 0, hop, batch, offset)
            forward(weight, 1, 1, hop, batch, offset)

    UP = (
        (1, (1, 0)),
        (2, (1, 1)),
        (3, (1, 2), (2, 0)),
        (4, (1, 3), (2, 1)),
        (5, (1, 4), (2, 2), (3, 0)),
        ((2, 3), (3, 1)),
        ((2, 4), (3, 2), (4, 0)),
        ((3, 3), (4, 1)),
        ((3, 4), (4, 2)),
        ((4, 3),),
        ((4, 4),),
    )
    DOWN = (
        (1, (1, 0)),
        (2, (1, 1)),
        (3, (2, 0)),
        ((1, 2), 4, (2, 1)),
        ((1, 3), (3, 0)),
        (5, (1, 4), (2, 2)),
        ((2, 3), (3, 1)),
        ((2, 4), (3, 2), (4, 0)),
        ((3, 3),),
        ((3, 4),),
        ((4, 1), (4, 2)),
        ((4, 3),),
        ((4, 4),),
    )

    def rounds(weight, items):
        for item in items:
            if isinstance(item, int):
                along(weight, item)
            else:
                across_to(weight, *item)

    def event(k):
        rounds(0, UP[k])

    def fill(k):
        rounds(1, DOWN[k])

    event(0)
    fill(0)
    up_all[z, y] = up[...]
    down_all[z, y] = down[...]

    ext[8 : 8 + ROWS, :] = inner[...].astype(F32)
    ext_c[8 : 8 + ROWS] = coeff[...].astype(F32)

    def taps(b):
        for j in range(4):
            if j < 2:
                lanes = slice(COLS * j, COLS * (j + 1))
                weights = taps_inner[:, lanes].astype(F32)
                shifted = lambda k: ext[pl.ds(b * BLOCK + 5 + k, BLOCK), lanes]
                target = lanes
            else:
                weights = taps_coeff[...].astype(F32)[:, j - 2, :]
                shifted = lambda k: ext_c[pl.ds(b * BLOCK + 5 + k, BLOCK), j - 2, :]
                target = slice(INNER + STATE * (j - 2), INNER + STATE * (j - 1))
            total_taps = shifted(0) * weights[0:1]
            for k in range(1, 4):
                total_taps = total_taps + shifted(k) * weights[k : k + 1]
            act[b * BLOCK : (b + 1) * BLOCK, target] = silu(total_taps).astype(BF)

    def block_state(b):
        rb = slice(b * BLOCK, (b + 1) * BLOCK)
        weight = step[rb, :] * jnp.exp(ends[b] - cum[rb, :])
        values = act[rb, 0:INNER].astype(F32) * per_head(weight)
        states[b] = dot(act[rb, INNER : INNER + STATE], values.astype(BF), TN)

    taps(1)
    taps(2)
    block_state(1)
    block_state(2)
    landed(inner_tail, hist_inner)
    landed(coeff_tail, hist_coeff)
    is_first = jnp.logical_and(z == 0, y == 0)
    ext[0:8, :] = jnp.where(is_first, 0.0, hist_inner[8:16, :].astype(F32))
    ext_c[0:8] = jnp.where(is_first, 0.0, hist_coeff[...].astype(F32))
    taps(0)
    block_state(0)
    own[...] = (
        states[0] * per_head(jnp.exp(ends[1] + ends[2])) + states[1] * per_head(jnp.exp(ends[2])) + states[2]
    ).astype(BF)

    slice_of = lambda v: pl.ds(pl.multiple_of(v * SLICE, SLICE), SLICE)
    st1_landed = to_all(lambda d: own.at[slice_of(at(y, d))], (st_row.at[y], st_row.at[seven]), along_y)
    event(1)
    fill(1)
    st_row[y] = own[slice_of(y), :]

    def inside(b):
        rb = slice(b * BLOCK, (b + 1) * BLOCK)
        scores = dot(act[rb, INNER + STATE :], act[rb, INNER : INNER + STATE], NT)
        for j in range(HEADS // 2):
            lanes = slice(128 * j, 128 * (j + 1))
            parts = []
            for h in (2 * j, 2 * j + 1):
                gap = cum[rb, h : h + 1] - cum_t[h : h + 1, rb]
                within = jnp.exp(jnp.where(causal, gap, -1e30)) * (scores * step_t[h : h + 1, rb])
                parts.append(dot(within.astype(BF), act[rb, lanes], NN))
            local[rb, lanes] = jnp.where(low_lanes, parts[0], parts[1])

    def carried(b):
        rb = slice(b * BLOCK, (b + 1) * BLOCK)
        if b == 1:
            inner_state = states[0]
        else:
            inner_state = states[0] * per_head(jnp.exp(ends[1])) + states[1]
        local[rb, :] += dot(act[rb, INNER + STATE :], inner_state.astype(BF), NN) * per_head(jnp.exp(cum[rb, :]))

    ld_landed()
    row_logs = ld_row[:, 0, :]
    ld_total[...] = jnp.broadcast_to(jnp.sum(row_logs, axis=0, keepdims=True), (8, 128))
    ld2_landed = to_all(lambda d: ld_total, (ld_rows.at[z], ld_rows.at[seven]), along_z)
    ld_rows[z] = ld_total[...]
    row_decay = per_head(jnp.exp(row_logs))

    inside(0)
    inside(1)
    inside(2)
    carried(1)
    carried(2)
    st1_landed()
    run = jnp.zeros((SLICE, INNER), F32)
    for k in range(N):
        pre[k] = run
        run = run * row_decay[k : k + 1, :] + st_row[k].astype(F32)
    st_total[...] = run.astype(BF)
    st2_landed = to_all(lambda d: st_total, (st_rows.at[z], st_rows.at[seven]), along_z)
    st_rows[z] = st_total[...]
    event(2)
    fill(2)
    ld2_landed()
    rows_decay = per_head(jnp.exp(ld_rows[:, 0, :]))
    st2_landed()
    run = jnp.zeros((SLICE, INNER), F32)
    for k in range(N):
        run = jnp.where(k < z, run * rows_decay[k : k + 1, :] + st_rows[k].astype(F32), run)
    for k in range(N):
        st_back[k] = (pre[k] + run).astype(BF)
        if k < N - 1:
            run = run * row_decay[k : k + 1, :]
    st3_landed = to_all(
        lambda d: st_back.at[at(y, d)], (enter.at[slice_of(y)], enter.at[pl.ds(0, SLICE * (N - 1))]), along_y
    )
    enter[slice_of(y), :] = st_back[y]

    event(3)
    fill(3)
    st3_landed()
    event(4)
    fill(4)
    mixer_gain_copy.wait()
    gate_copy.wait()
    start_log = jnp.zeros_like(ends[0])
    for b in range(NB):
        rb = slice(b * BLOCK, (b + 1) * BLOCK)
        outer = dot(act[rb, INNER + STATE :], enter[...], NN) * per_head(jnp.exp(cum[rb, :] + start_log))
        gated = (local[rb, :] + outer) * silu(gate[rb, :].astype(F32))
        mean = jnp.mean(gated * gated, axis=1, keepdims=True)
        mixed[rb, :] = (gated * lax.rsqrt(mean + EPS) * mixer_gain[...]).astype(BF)
        start_log = start_log + ends[b]

    top, bottom = pl.ds(0, HALF), pl.ds(HALF, HALF)

    class Reduction:
        def __init__(self, block, refs):
            self.block = block
            self.pair_out, self.pair_in, self.far, self.relay, self.near, self.fin, self.keep = refs
            self.pair_sent, self.ring_sent = sender(self.pair_in), sender(self.pair_in.at[pl.ds(0, 3)])
            self.pair_landed = [receiver() for _ in range(NX)]
            self.from_l, self.from_r, self.final = receiver(), receiver(), receiver()

        def both(self, *members):
            value = self.block(*[atx((2, 1, 3, 0)[i]) for i in members])
            width = value.shape[1] // len(members)
            for n, i in enumerate(members):
                self.share(i, value[:, n * width : (n + 1) * width])

        def share(self, i, value):
            width = value.shape[1] // 2
            lower, upper = value[:, :width], value[:, width:]
            self.pair_out[i] = jnp.where(c == 0, upper, lower).astype(BF)
            go(self.pair_out.at[i], self.pair_in.at[i], partner, self.pair_sent, self.pair_landed[i])
            self.keep[i] = jnp.where(c == 0, lower, upper)

        def mine(self, i):
            landed(self.pair_landed[i], self.pair_in.at[i])
            return self.keep[i] + self.pair_in[i].astype(F32)

        def send_far(self):
            self.far[...] = self.mine(0).astype(BF)
            go(self.far.at[top], self.relay.at[0], right, self.ring_sent, self.from_l)
            go(self.far.at[bottom], self.relay.at[1], left, self.ring_sent, self.from_r)

        def send_right(self):
            self.keep[1] = value = self.mine(1)
            self.near[0, HALF:, :] = value[HALF:].astype(BF)
            go(self.near.at[0, bottom], self.fin.at[0, bottom], right, self.ring_sent, self.final)

        def send_left(self):
            self.keep[2] = value = self.mine(2)
            self.near[1, :HALF, :] = value[:HALF].astype(BF)
            go(self.near.at[1, top], self.fin.at[1, top], left, self.ring_sent, self.final)

        def own(self):
            self.keep[3] = self.mine(3)

        def pass_on(self):
            landed(self.from_l, self.relay.at[0])
            self.near[0, :HALF, :] = (self.keep[1, :HALF, :] + self.relay[0].astype(F32)).astype(BF)
            go(self.near.at[0, top], self.fin.at[0, top], right, self.ring_sent, self.final)
            landed(self.from_r, self.relay.at[1])
            self.near[1, HALF:, :] = (self.keep[2, HALF:, :] + self.relay[1].astype(F32)).astype(BF)
            go(self.near.at[1, bottom], self.fin.at[1, bottom], left, self.ring_sent, self.final)

        def total(self):
            landed(self.final, self.fin)
            return self.keep[3] + self.fin[0].astype(F32) + self.fin[1].astype(F32)

    def out_block(chip):
        return dot(mixed[...], out_w[:, pl.ds(pl.multiple_of(chip * 2 * COLS, 2 * COLS), 2 * COLS)], NN)

    out_copy.wait()
    mixer_sum = Reduction(out_block, reductions[0:7])
    mixer_sum.both(0)
    mixer_sum.both(1)
    mixer_sum.send_far()
    mixer_sum.both(2)
    mixer_sum.send_right()
    mixer_sum.both(3)
    mixer_sum.send_left()
    mixer_sum.own()
    event(5)
    fill(5)
    mixer_sum.pass_on()
    event(6)
    fill(6)
    projected = mixer_sum.total()
    residual_copy.wait()
    first[...] = (residual[...].astype(F32) + projected).astype(BF)
    rows[tp] = first[...]

    mine_tp, left_tp, right_tp, far_tp = tp, 2 * atx(3) + c, 2 * atx(1) + c, 2 * atx(2) + c
    rows_sent = sender(rows.at[seven])
    l_first, r_first, l_second, r_second, far_landed, across_landed = (receiver() for _ in range(6))
    go(first.at[top], rows.at[tp, top], right, rows_sent, l_first)
    go(first.at[bottom], rows.at[tp, bottom], left, rows_sent, r_first)
    go(first, rows.at[tp], partner, rows_sent, across_landed)
    go(first.at[bottom], rows.at[tp, bottom], right, rows_sent, l_second)
    go(first.at[top], rows.at[tp, top], left, rows_sent, r_second)
    event(7)
    fill(7)
    gain_landed()
    squares = jnp.zeros((ROWS, 1), F32)

    def raise_rows(source, squares, new=False):
        wide = rows[source].astype(F32)
        squares = squares + jnp.sum(wide * wide, axis=1, keepdims=True)
        scaled = (wide * gain_all[source][0:1, :]).astype(BF)
        weights = up_all[source].reshape(COLS, FF)
        product = dot(scaled, weights, NN)
        acc[...] = product if new else acc[...] + product
        return squares

    half_rows = rows.at[0, top]
    landed(l_first, half_rows)
    go(rows.at[left_tp, top], rows.at[left_tp, top], right, rows_sent, far_landed)
    landed(r_first, half_rows)
    go(rows.at[right_tp, bottom], rows.at[right_tp, bottom], left, rows_sent, far_landed)
    event(8)
    fill(8)
    landed(l_second, half_rows)
    go(rows.at[left_tp], rows.at[left_tp], partner, rows_sent, across_landed)
    landed(r_second, half_rows)
    go(rows.at[right_tp], rows.at[right_tp], partner, rows_sent, across_landed)
    event(9)
    fill(9)
    landed(far_landed, rows.at[0])
    go(rows.at[far_tp], rows.at[far_tp], partner, rows_sent, across_landed)
    event(10)
    fill(10)
    landed(across_landed, rows.at[pl.ds(0, NX)])
    fill(11)
    for batch in range(5):
        pieces_landed(0, 1, 4, batch)
    fill(12)
    for k in range(N):
        squares = raise_rows(k, squares, k == 0)
    scale = lax.rsqrt(squares * (1.0 / D) + EPS)
    active[...] = jnp.square(jnp.maximum(acc[...] * scale, 0.0)).astype(BF)

    def down_block(half):
        def block(*chips):
            pieces = [
                down_all[2 * chip + j, at(y, (N - 1 + 4 * half + p) % N)]
                for chip in chips
                for j in range(2)
                for p in range(4)
            ]
            return dot(active[...], jnp.concatenate(pieces, axis=0), NT)

        return block

    early, late = Reduction(down_block(0), reductions[7:14]), Reduction(down_block(1), reductions[14:21])
    for batch in range(3):
        pieces_landed(1, 1, 4, batch)
    early.both(0, 1)
    early.both(2, 3)
    early.send_far()
    early.send_right()
    early.send_left()
    for batch in range(3, 5):
        pieces_landed(1, 1, 4, batch)
    late.both(0, 1)
    early.own()
    late.both(2, 3)
    late.send_far()
    early.pass_on()
    late.send_right()
    late.send_left()
    late.own()
    late.pass_on()
    turned = early.total()
    turned = jnp.concatenate([turned, late.total()], axis=1)
    lowered = pltpu.roll(turned, at(y, N - 1) * PIECE, 1)
    result[...] = (first[...].astype(F32) + lowered).astype(BF)
    for sent, total in pending:
        remote(total, total, partner, sent, recv.at[0]).wait_send()


def shards(
    inner_pre, coeff_pre, gate_pre, step_raw, step_bias, decay_log, conv_inner, conv_coeff, mixer_gain,
    out_weight, residual, mlp_gain, up_weight, down_weight,
):
    vm = pltpu.VMEM
    dma = pltpu.SemaphoreType.DMA
    scratch = [
        vm((ROWS, INNER), BF), vm((ROWS, 2, STATE), BF), vm((ROWS, INNER), BF), vm((ROWS, COLS), BF),
        vm((PIECE, FF), BF), vm((PIECE, FF), BF), vm((HEADS, ROWS), BF), vm((1, HEADS), F32), vm((1, HEADS), F32),
        vm((4, INNER), BF), vm((4, 2, STATE), BF), vm((1, INNER), F32), vm((1, COLS), F32),
        vm((EDGE, INNER), BF), vm((8, 2, STATE), BF), vm((ROWS + 8, INNER), F32), vm((ROWS + 8, 2, STATE), F32), vm((ROWS, INNER + COLS), BF),
        vm((ROWS, HEADS), F32), vm((HEADS, ROWS), F32), vm((ROWS, HEADS), F32), vm((HEADS, ROWS), F32),
        vm((ROWS, INNER), F32), vm((NB, STATE, INNER), F32), vm((STATE, INNER), BF), vm((STATE, INNER), BF),
        vm((8, 128), F32), vm((N, 8, 128), F32), vm((8, 128), F32), vm((N, 8, 128), F32),
        vm((N, SLICE, INNER), F32), vm((N, SLICE, INNER), BF), vm((SLICE, INNER), BF), vm((N, SLICE, INNER), BF),
        vm((N, SLICE, INNER), BF),
        vm((ROWS, INNER), BF), vm((INNER, D), BF), vm((N, N, PIECE, FF), BF), vm((N, N, PIECE, FF), BF),
        vm((8, COLS), F32), vm((N, 8, COLS), F32),
        vm((N, ROWS, COLS), BF), vm((ROWS, COLS), BF), vm((ROWS, FF), F32), vm((ROWS, FF), BF),
        dma((19,)), dma((83,)), dma((14,)),
    ]
    for width in (COLS, COLS // 2, COLS // 2):
        scratch += [
            vm((NX, ROWS, width), BF), vm((NX, ROWS, width), BF), vm((ROWS, width), BF), vm((2, HALF, width), BF),
            vm((2, ROWS, width), BF), vm((2, ROWS, width), BF), vm((NX, ROWS, width), F32),
        ]
    return pl.pallas_call(
        kernel,
        out_shape=pltpu.VMEM((ROWS, COLS), BF),
        in_specs=[pl.BlockSpec(memory_space=pltpu.HBM)] * 14,
        out_specs=pl.BlockSpec(memory_space=pltpu.VMEM),
        scratch_shapes=scratch,
        compiler_params=pltpu.CompilerParams(
            collective_id=0, has_side_effects=True, vmem_limit_bytes=60 * 1024 * 1024
        ),
        name="layer",
    )(
        inner_pre, coeff_pre, gate_pre, step_raw.T, step_bias[None], decay_log[None], conv_inner,
        conv_coeff, mixer_gain[None], out_weight, residual, mlp_gain[None], up_weight, down_weight.T,
    )


def solution(mesh):
    split = Mesh(mesh.devices.reshape(N, N, NX, 2), ("z", "y", "x", "c"))
    sp, tp = ("z", "y"), ("x", "c")
    return jax.shard_map(
        shards,
        mesh=split,
        in_specs=(
            P(sp, tp), P(sp, None, tp), P(sp, tp), P(sp, tp), P(tp), P(tp), P(None, tp), P(None, None, tp), P(tp),
            P(tp, None), P(sp, tp), P(tp), P(sp, tp), P(tp, sp),
        ),
        out_specs=P(sp, tp),
        check_vma=False,
    )
```

```python
import jax
import jax.numpy as jnp
from jax import lax
from jax.experimental import pallas as pl
from jax.experimental.pallas import tpu as pltpu
from jax.sharding import Mesh
from jax.sharding import PartitionSpec as P

MESH = pl.DeviceIdType.MESH
BF = jnp.bfloat16
F32 = jnp.float32
HIGH = lax.Precision.HIGHEST
EPS = 1e-05

ROWS = 384
HALF = ROWS // 2
BLOCK = 128
NB = ROWS // BLOCK
INNER = 512
STATE = 128
HEADS = 8
COLS = 256
FF = 1024
D = 2048
N = 8
NX = 4
PIECE = 32
SLICE = STATE // N
EDGE = 16


def dot(a, b, dims, precision=None):
    return lax.dot_general(a, b, (dims, ((), ())), precision=precision, preferred_element_type=F32)


NN = ((1,), (0,))
NT = ((1,), (1,))
TN = ((0,), (0,))


def per_head(v):
    low = lax.broadcasted_iota(jnp.int32, (v.shape[0], 128), 1) < 64
    tiles = [jnp.where(low, v[:, 2 * j : 2 * j + 1], v[:, 2 * j + 1 : 2 * j + 2]) for j in range(HEADS // 2)]
    return jnp.concatenate(tiles, axis=1)


def silu(v):
    return v / (1.0 + jnp.exp(-v))


def kernel(
    inner_hbm, coeff_hbm, gate_hbm, step_raw_hbm, step_bias_hbm, decay_log_hbm, taps_inner_hbm, taps_coeff_hbm,
    mixer_gain_hbm, out_hbm, residual_hbm, mlp_gain_hbm, up_hbm, down_hbm, result,
    inner, coeff, gate, residual, up, down, step_raw, step_bias, decay_log, taps_inner, taps_coeff, mixer_gain,
    mlp_gain,
    hist_inner, hist_coeff, ext, ext_c, act, cum, cum_t, step, step_t, local, states, own, enter,
    ld_own, ld_row, ld_total, ld_rows, pre, st_row, st_total, st_rows, st_back,
    mixed, out_w, up_all, down_all, gain_own, gain_all,
    rows, first, acc, active, send, recv, local_sem, *reductions,
):
    z, y, x, c = (lax.axis_index(a) for a in ("z", "y", "x", "c"))
    tp = 2 * x + c
    at = lambda v, d: lax.rem(v + d, N)
    atx = lambda d: lax.rem(x + d, NX)
    next_id = {"z": at(z, jnp.where(y == N - 1, 1, 0)), "y": at(y, 1)}
    prev_id = {"z": at(z, jnp.where(y == 0, N - 1, 0)), "y": at(y, N - 1)}
    right, left = {"x": atx(1)}, {"x": atx(NX - 1)}
    partner = {"c": 1 - c}
    tp_id = lambda d: {"x": at(tp, d) // 2, "c": lax.rem(at(tp, d), 2)}

    barrier = pltpu.get_barrier_semaphore()
    greeted = [next_id, prev_id]
    for d in range(1, N):
        greeted += [{"y": at(y, d)}, {"z": at(z, d)}, tp_id(d)]
    for where in greeted:
        pl.semaphore_signal(barrier, inc=1, device_id=where, device_id_type=MESH)

    fetched = [
        pltpu.make_async_copy(there, here, local_sem.at[i])
        for i, (there, here) in enumerate(
            (
                (step_raw_hbm, step_raw), (step_bias_hbm, step_bias), (decay_log_hbm, decay_log),
                (mlp_gain_hbm, mlp_gain), (taps_inner_hbm, taps_inner), (taps_coeff_hbm, taps_coeff),
                (up_hbm, up), (down_hbm, down), (inner_hbm, inner), (coeff_hbm, coeff),
                (mixer_gain_hbm, mixer_gain), (gate_hbm, gate), (residual_hbm, residual), (out_hbm, out_w),
            )
        )
    ]
    for copy in fetched:
        copy.start()
    up_copy, down_copy, inner_copy, coeff_copy, mixer_gain_copy, gate_copy, residual_copy, out_copy = fetched[6:]

    used = [0, 0]
    pending = []

    def remote(src, dst, where, sent, arrived):
        return pltpu.make_async_remote_copy(
            src_ref=src, dst_ref=dst, send_sem=sent, recv_sem=arrived, device_id=where, device_id_type=MESH
        )

    def sender(total):
        used[0] += 1
        pending.append((send.at[used[0] - 1], total))
        return send.at[used[0] - 1]

    def receiver():
        used[1] += 1
        return recv.at[used[1] - 1]

    def go(*args):
        remote(*args).start()

    def landed(arrived, total):
        remote(total, total, partner, send.at[0], arrived).wait_recv()

    row_i = lax.broadcasted_iota(jnp.int32, (BLOCK, BLOCK), 0)
    col_i = lax.broadcasted_iota(jnp.int32, (BLOCK, BLOCK), 1)
    causal = row_i >= col_i
    tril = causal.astype(F32)
    triu = (row_i <= col_i).astype(F32)
    eye = (row_i == col_i).astype(F32)
    low_lanes = col_i < 64

    on_heads = lax.broadcasted_iota(jnp.int32, (HEADS, HEADS), 0) == lax.broadcasted_iota(jnp.int32, (HEADS, HEADS), 1)
    column = lambda v: jnp.sum(jnp.where(on_heads, jnp.broadcast_to(v, (HEADS, HEADS)), 0.0), axis=1, keepdims=True)
    for copy in fetched[:6]:
        copy.wait()
    bias = column(step_bias[...])
    rate = jnp.exp(column(decay_log[...]))
    ends = []
    for b in range(NB):
        rb = pl.ds(b * BLOCK, BLOCK)
        raw = step_raw[:, rb].astype(F32) + bias
        size = jnp.maximum(raw, 0.0) + jnp.log1p(jnp.exp(-jnp.abs(raw)))
        logs = -size * rate
        cum_b = dot(tril, logs, NT, HIGH)
        cum[rb, :] = cum_b
        cum_t[:, rb] = dot(logs, triu, NN, HIGH)
        step[rb, :] = dot(eye, size, NT, HIGH)
        step_t[:, rb] = size
        ends.append(cum_b[BLOCK - 1 : BLOCK, :])
    total = ends[0] + ends[1] + ends[2]
    ld_own[...] = jnp.zeros_like(ld_own)
    ld_own[:, 0:HEADS] = total
    gain_own[...] = jnp.broadcast_to(mlp_gain[...], gain_own.shape)

    pl.semaphore_wait(barrier, len(greeted))

    inner_copy.wait()
    coeff_copy.wait()
    inner_tail, coeff_tail = receiver(), receiver()
    go(inner.at[pl.ds(ROWS - EDGE, EDGE)], hist_inner, next_id, sender(hist_inner), inner_tail)
    go(coeff.at[pl.ds(ROWS - 8, 8)], hist_coeff, next_id, sender(hist_coeff), coeff_tail)
    seven = pl.ds(0, N - 1)

    def to_all(source, target, where):
        sent, arrived = sender(target[1]), receiver()
        for d in range(1, N):
            go(source(d), target[0], where(d), sent, arrived)
        return lambda: landed(arrived, target[1])

    along_y, along_z = lambda d: {"y": at(y, d)}, lambda d: {"z": at(z, d)}
    ld_landed = to_all(lambda d: ld_own, (ld_row.at[y], ld_row.at[seven]), along_y)
    gain_landed = to_all(lambda d: gain_own, (gain_all.at[tp], gain_all.at[seven]), tp_id)
    ld_row[y] = ld_own[...]
    gain_all[tp] = gain_own[...]

    up_copy.wait()
    down_copy.wait()
    OFFSETS = ((0,), (N - 1, 1), (N - 2, 2), (N - 3, 3), (4,))
    weights_sent = [[sender(w.at[0, seven]), sender(w.at[seven])] for w in (up_all, down_all)]
    weights_landed = [
        [[receiver() for _ in range(4)], [[receiver() for _ in range(5)] for _ in range(4)]] for _ in range(2)
    ]

    def forward(weight, stage, way, hop, batch=0, offset=0):
        back = (N - (hop - 1)) % N if way == 0 else hop - 1
        to = 1 if way == 0 else N - 1
        whole, piece = (up_all, up) if weight == 0 else (down_all, down)
        arrived = weights_landed[weight][stage][hop - 1]
        arrived = arrived if stage == 0 else arrived[batch]
        columns = slice(None) if hop < 4 else pl.ds(way * (FF // 2), FF // 2)
        for order in range(2):
            part = pl.ds(order * (PIECE // 2), PIECE // 2)
            a, b = (z, y) if order == 0 else (y, z)
            if stage == 0:
                ia, ib = at(a, back), b
            else:
                ia, ib = at(a, offset), at(b, back)
            on_z = (stage == 0) == (order == 0)
            where = {"z": at(z, to)} if on_z else {"y": at(y, to)}
            iz, iy = (ia, ib) if order == 0 else (ib, ia)
            ref = whole.at[iz, iy, part, columns]
            source = piece.at[part] if hop == 1 and offset == 0 else ref
            go(source, ref, where, weights_sent[weight][stage], arrived)

    def pieces_landed(weight, stage, hop, batch=0):
        count = len(OFFSETS[batch]) * (1 if hop == 4 else 2)
        arrived = weights_landed[weight][stage][hop - 1]
        if stage == 0:
            arrived, count = arrived, 1 if hop == 4 else 2
        else:
            arrived = arrived[batch]
        landed(arrived, (up_all if weight == 0 else down_all).at[0, pl.ds(0, count)])

    def along(weight, hop):
        if hop > 1:
            pieces_landed(weight, 0, hop - 1)
        if hop < 5:
            forward(weight, 0, 0, hop)
            forward(weight, 0, 1, hop)

    def across_to(weight, hop, batch):
        if hop > 1:
            pieces_landed(weight, 1, hop - 1, batch)
        for offset in OFFSETS[batch]:
            forward(weight, 1, 0, hop, batch, offset)
            forward(weight, 1, 1, hop, batch, offset)

    UP = (
        (1, (1, 0)),
        (2, (1, 1)),
        (3, (1, 2), (2, 0)),
        (4, (1, 3), (2, 1)),
        (5, (1, 4), (2, 2), (3, 0)),
        ((2, 3), (3, 1)),
        ((2, 4), (3, 2), (4, 0)),
        ((3, 3), (4, 1)),
        ((3, 4), (4, 2)),
        ((4, 3),),
        ((4, 4),),
    )
    DOWN = (
        (1, (1, 0)),
        (2, (1, 1)),
        (3, (2, 0)),
        ((1, 2), 4, (2, 1)),
        ((1, 3), (3, 0)),
        (5, (1, 4), (2, 2)),
        ((2, 3), (3, 1)),
        ((2, 4),),
        ((3, 2), (3, 3)),
        ((3, 4), (4, 0)),
        ((4, 1), (4, 2)),
        ((4, 3),),
        ((4, 4),),
    )

    def rounds(weight, items):
        for item in items:
            if isinstance(item, int):
                along(weight, item)
            else:
                across_to(weight, *item)

    def event(k):
        rounds(0, UP[k])

    def fill(k):
        rounds(1, DOWN[k])

    event(0)
    fill(0)
    up_all[z, y] = up[...]
    down_all[z, y] = down[...]

    ext[8 : 8 + ROWS, :] = inner[...].astype(F32)
    ext_c[8 : 8 + ROWS] = coeff[...].astype(F32)

    ext[0:8, :] = jnp.zeros((8, INNER), F32)
    ext_c[0:8] = jnp.zeros((8, 2, STATE), F32)

    def taps(b, count=BLOCK):
        for j in range(4):
            if j < 2:
                lanes = slice(COLS * j, COLS * (j + 1))
                weights = taps_inner[:, lanes].astype(F32)
                shifted = lambda k: ext[pl.ds(b * BLOCK + 5 + k, count), lanes]
                target = lanes
            else:
                weights = taps_coeff[...].astype(F32)[:, j - 2, :]
                shifted = lambda k: ext_c[pl.ds(b * BLOCK + 5 + k, count), j - 2, :]
                target = slice(INNER + STATE * (j - 2), INNER + STATE * (j - 1))
            total_taps = shifted(0) * weights[0:1]
            for k in range(1, 4):
                total_taps = total_taps + shifted(k) * weights[k : k + 1]
            act[b * BLOCK : b * BLOCK + count, target] = silu(total_taps).astype(BF)

    def block_state(b):
        rb = slice(b * BLOCK, (b + 1) * BLOCK)
        weight = step[rb, :] * jnp.exp(ends[b] - cum[rb, :])
        values = act[rb, 0:INNER].astype(F32) * per_head(weight)
        states[b] = dot(act[rb, INNER : INNER + STATE], values.astype(BF), TN)

    taps(1)
    taps(2)
    block_state(1)
    block_state(2)
    taps(0)
    landed(inner_tail, hist_inner)
    landed(coeff_tail, hist_coeff)
    is_first = jnp.logical_and(z == 0, y == 0)
    ext[0:8, :] = jnp.where(is_first, 0.0, hist_inner[8:16, :].astype(F32))
    ext_c[0:8] = jnp.where(is_first, 0.0, hist_coeff[...].astype(F32))
    taps(0, EDGE)
    block_state(0)
    own[...] = (
        states[0] * per_head(jnp.exp(ends[1] + ends[2])) + states[1] * per_head(jnp.exp(ends[2])) + states[2]
    ).astype(BF)

    slice_of = lambda v: pl.ds(pl.multiple_of(v * SLICE, SLICE), SLICE)
    st1_landed = to_all(lambda d: own.at[slice_of(at(y, d))], (st_row.at[y], st_row.at[seven]), along_y)
    event(1)
    fill(1)
    st_row[y] = own[slice_of(y), :]

    def inside(b):
        rb = slice(b * BLOCK, (b + 1) * BLOCK)
        scores = dot(act[rb, INNER + STATE :], act[rb, INNER : INNER + STATE], NT)
        for j in range(HEADS // 2):
            lanes = slice(128 * j, 128 * (j + 1))
            parts = []
            for h in (2 * j, 2 * j + 1):
                gap = cum[rb, h : h + 1] - cum_t[h : h + 1, rb]
                within = jnp.exp(jnp.where(causal, gap, -1e30)) * (scores * step_t[h : h + 1, rb])
                parts.append(dot(within.astype(BF), act[rb, lanes], NN))
            local[rb, lanes] = jnp.where(low_lanes, parts[0], parts[1])

    def carried(b):
        rb = slice(b * BLOCK, (b + 1) * BLOCK)
        if b == 1:
            inner_state = states[0]
        else:
            inner_state = states[0] * per_head(jnp.exp(ends[1])) + states[1]
        local[rb, :] += dot(act[rb, INNER + STATE :], inner_state.astype(BF), NN) * per_head(jnp.exp(cum[rb, :]))

    ld_landed()
    row_logs = ld_row[:, 0, :]
    ld_total[...] = jnp.sum(row_logs, axis=0, keepdims=True)
    ld2_landed = to_all(lambda d: ld_total, (ld_rows.at[z], ld_rows.at[seven]), along_z)
    ld_rows[z] = ld_total[...]
    row_decay = per_head(jnp.exp(row_logs))

    inside(0)
    inside(1)
    inside(2)
    carried(1)
    carried(2)
    st1_landed()
    run = jnp.zeros((SLICE, INNER), F32)
    for k in range(N):
        pre[k] = run
        run = run * row_decay[k : k + 1, :] + st_row[k].astype(F32)
    st_total[...] = run.astype(BF)
    st2_landed = to_all(lambda d: st_total, (st_rows.at[z], st_rows.at[seven]), along_z)
    st_rows[z] = st_total[...]
    event(2)
    fill(2)
    ld2_landed()
    rows_decay = per_head(jnp.exp(ld_rows[:, 0, :]))
    st2_landed()
    run = jnp.zeros((SLICE, INNER), F32)
    for k in range(N):
        run = jnp.where(k < z, run * rows_decay[k : k + 1, :] + st_rows[k].astype(F32), run)
    for k in range(N):
        st_back[k] = (pre[k] + run).astype(BF)
        if k < N - 1:
            run = run * row_decay[k : k + 1, :]
    st3_landed = to_all(
        lambda d: st_back.at[at(y, d)], (enter.at[slice_of(y)], enter.at[pl.ds(0, SLICE * (N - 1))]), along_y
    )
    enter[slice_of(y), :] = st_back[y]

    event(3)
    fill(3)
    st3_landed()
    event(4)
    fill(4)
    mixer_gain_copy.wait()
    gate_copy.wait()
    start_log = jnp.zeros_like(ends[0])
    for b in range(NB):
        rb = slice(b * BLOCK, (b + 1) * BLOCK)
        outer = dot(act[rb, INNER + STATE :], enter[...], NN) * per_head(jnp.exp(cum[rb, :] + start_log))
        gated = (local[rb, :] + outer) * silu(gate[rb, :].astype(F32))
        mean = jnp.mean(gated * gated, axis=1, keepdims=True)
        mixed[rb, :] = (gated * lax.rsqrt(mean + EPS) * mixer_gain[...]).astype(BF)
        start_log = start_log + ends[b]

    top, bottom = pl.ds(0, HALF), pl.ds(HALF, HALF)

    class Reduction:
        def __init__(self, block, refs):
            self.block = block
            self.pair_out, self.pair_in, self.far, self.relay, self.near, self.fin, self.keep = refs
            self.pair_sent, self.ring_sent = sender(self.pair_in), sender(self.pair_in.at[pl.ds(0, 3)])
            self.pair_landed = [receiver() for _ in range(NX)]
            self.from_l, self.from_r, self.final = receiver(), receiver(), receiver()

        def both(self, *members):
            value = self.block(*[atx((2, 1, 3, 0)[i]) for i in members])
            width = value.shape[1] // len(members)
            for n, i in enumerate(members):
                self.share(i, value[:, n * width : (n + 1) * width])

        def share(self, i, value):
            width = value.shape[1] // 2
            lower, upper = value[:, :width], value[:, width:]
            self.pair_out[i] = jnp.where(c == 0, upper, lower).astype(BF)
            go(self.pair_out.at[i], self.pair_in.at[i], partner, self.pair_sent, self.pair_landed[i])
            self.keep[i] = jnp.where(c == 0, lower, upper)

        def mine(self, i):
            landed(self.pair_landed[i], self.pair_in.at[i])
            return self.keep[i] + self.pair_in[i].astype(F32)

        def send_far(self):
            self.far[...] = self.mine(0).astype(BF)
            go(self.far.at[top], self.relay.at[0], right, self.ring_sent, self.from_l)
            go(self.far.at[bottom], self.relay.at[1], left, self.ring_sent, self.from_r)

        def send_right(self):
            self.keep[1] = value = self.mine(1)
            self.near[0, HALF:, :] = value[HALF:].astype(BF)
            go(self.near.at[0, bottom], self.fin.at[0, bottom], right, self.ring_sent, self.final)

        def send_left(self):
            self.keep[2] = value = self.mine(2)
            self.near[1, :HALF, :] = value[:HALF].astype(BF)
            go(self.near.at[1, top], self.fin.at[1, top], left, self.ring_sent, self.final)

        def own(self):
            self.keep[3] = self.mine(3)

        def pass_on(self):
            landed(self.from_l, self.relay.at[0])
            self.near[0, :HALF, :] = (self.keep[1, :HALF, :] + self.relay[0].astype(F32)).astype(BF)
            go(self.near.at[0, top], self.fin.at[0, top], right, self.ring_sent, self.final)
            landed(self.from_r, self.relay.at[1])
            self.near[1, HALF:, :] = (self.keep[2, HALF:, :] + self.relay[1].astype(F32)).astype(BF)
            go(self.near.at[1, bottom], self.fin.at[1, bottom], left, self.ring_sent, self.final)

        def total(self):
            landed(self.final, self.fin)
            return self.keep[3] + self.fin[0].astype(F32) + self.fin[1].astype(F32)

    def out_block(chip):
        return dot(mixed[...], out_w[:, pl.ds(pl.multiple_of(chip * 2 * COLS, 2 * COLS), 2 * COLS)], NN)

    out_copy.wait()
    mixer_sum = Reduction(out_block, reductions[0:7])
    mixer_sum.both(0)
    mixer_sum.both(1)
    mixer_sum.send_far()
    mixer_sum.both(2)
    mixer_sum.send_right()
    mixer_sum.both(3)
    mixer_sum.send_left()
    mixer_sum.own()
    event(5)
    fill(5)
    mixer_sum.pass_on()
    event(6)
    fill(6)
    projected = mixer_sum.total()
    residual_copy.wait()
    first[...] = (residual[...].astype(F32) + projected).astype(BF)
    rows[tp] = first[...]

    mine_tp, left_tp, right_tp, far_tp = tp, 2 * atx(3) + c, 2 * atx(1) + c, 2 * atx(2) + c
    rows_sent = sender(rows.at[seven])
    l_first, r_first, l_second, r_second, far_landed, across_landed = (receiver() for _ in range(6))
    go(first.at[top], rows.at[tp, top], right, rows_sent, l_first)
    go(first.at[bottom], rows.at[tp, bottom], left, rows_sent, r_first)
    go(first, rows.at[tp], partner, rows_sent, across_landed)
    go(first.at[bottom], rows.at[tp, bottom], right, rows_sent, l_second)
    go(first.at[top], rows.at[tp, top], left, rows_sent, r_second)
    event(7)
    fill(7)
    gain_landed()
    squares = jnp.zeros((ROWS, 1), F32)

    def raise_rows(source, squares, new=False):
        wide = rows[source].astype(F32)
        squares = squares + jnp.sum(wide * wide, axis=1, keepdims=True)
        scaled = (wide * gain_all[source][0:1, :]).astype(BF)
        weights = up_all[source].reshape(COLS, FF)
        product = dot(scaled, weights, NN)
        acc[...] = product if new else acc[...] + product
        return squares

    half_rows = rows.at[0, top]
    landed(l_first, half_rows)
    go(rows.at[left_tp, top], rows.at[left_tp, top], right, rows_sent, far_landed)
    landed(r_first, half_rows)
    go(rows.at[right_tp, bottom], rows.at[right_tp, bottom], left, rows_sent, far_landed)
    event(8)
    fill(8)
    landed(l_second, half_rows)
    go(rows.at[left_tp], rows.at[left_tp], partner, rows_sent, across_landed)
    landed(r_second, half_rows)
    go(rows.at[right_tp], rows.at[right_tp], partner, rows_sent, across_landed)
    event(9)
    landed(far_landed, rows.at[0])
    go(rows.at[far_tp], rows.at[far_tp], partner, rows_sent, across_landed)
    event(10)
    fill(9)
    fill(10)
    landed(across_landed, rows.at[pl.ds(0, NX)])
    fill(11)
    for batch in range(5):
        pieces_landed(0, 1, 4, batch)
    for k in range(N):
        squares = raise_rows(k, squares, k == 0)
        if k == 2:
            fill(12)
    scale = lax.rsqrt(squares * (1.0 / D) + EPS)
    active[...] = jnp.square(jnp.maximum(acc[...] * scale, 0.0)).astype(BF)

    def down_block(half):
        def block(*chips):
            pieces = [
                down_all[2 * chip + j, at(y, (N - 1 + 4 * half + p) % N)]
                for chip in chips
                for j in range(2)
                for p in range(4)
            ]
            return dot(active[...], jnp.concatenate(pieces, axis=0), NT)

        return block

    early, late = Reduction(down_block(0), reductions[7:14]), Reduction(down_block(1), reductions[14:21])
    for batch in range(3):
        pieces_landed(1, 1, 4, batch)
    early.both(0, 1)
    early.both(2, 3)
    early.send_far()
    early.send_right()
    early.send_left()
    for batch in range(3, 5):
        pieces_landed(1, 1, 4, batch)
    late.both(0, 1)
    early.own()
    late.both(2, 3)
    late.send_far()
    early.pass_on()
    late.send_right()
    late.send_left()
    late.own()
    late.pass_on()
    turned = early.total()
    turned = jnp.concatenate([turned, late.total()], axis=1)
    lowered = pltpu.roll(turned, at(y, N - 1) * PIECE, 1)
    result[...] = (first[...].astype(F32) + lowered).astype(BF)
    for sent, total in pending:
        remote(total, total, partner, sent, recv.at[0]).wait_send()


def shards(
    inner_pre, coeff_pre, gate_pre, step_raw, step_bias, decay_log, conv_inner, conv_coeff, mixer_gain,
    out_weight, residual, mlp_gain, up_weight, down_weight,
):
    vm = pltpu.VMEM
    dma = pltpu.SemaphoreType.DMA
    scratch = [
        vm((ROWS, INNER), BF), vm((ROWS, 2, STATE), BF), vm((ROWS, INNER), BF), vm((ROWS, COLS), BF),
        vm((PIECE, FF), BF), vm((PIECE, FF), BF), vm((HEADS, ROWS), BF), vm((1, HEADS), F32), vm((1, HEADS), F32),
        vm((4, INNER), BF), vm((4, 2, STATE), BF), vm((1, INNER), F32), vm((1, COLS), F32),
        vm((EDGE, INNER), BF), vm((8, 2, STATE), BF), vm((ROWS + 8, INNER), F32), vm((ROWS + 8, 2, STATE), F32), vm((ROWS, INNER + COLS), BF),
        vm((ROWS, HEADS), F32), vm((HEADS, ROWS), F32), vm((ROWS, HEADS), F32), vm((HEADS, ROWS), F32),
        vm((ROWS, INNER), F32), vm((NB, STATE, INNER), F32), vm((STATE, INNER), BF), vm((STATE, INNER), BF),
        vm((1, 128), F32), vm((N, 1, 128), F32), vm((1, 128), F32), vm((N, 1, 128), F32),
        vm((N, SLICE, INNER), F32), vm((N, SLICE, INNER), BF), vm((SLICE, INNER), BF), vm((N, SLICE, INNER), BF),
        vm((N, SLICE, INNER), BF),
        vm((ROWS, INNER), BF), vm((INNER, D), BF), vm((N, N, PIECE, FF), BF), vm((N, N, PIECE, FF), BF),
        vm((8, COLS), F32), vm((N, 8, COLS), F32),
        vm((N, ROWS, COLS), BF), vm((ROWS, COLS), BF), vm((ROWS, FF), F32), vm((ROWS, FF), BF),
        dma((19,)), dma((83,)), dma((14,)),
    ]
    for width in (COLS, COLS // 2, COLS // 2):
        scratch += [
            vm((NX, ROWS, width), BF), vm((NX, ROWS, width), BF), vm((ROWS, width), BF), vm((2, HALF, width), BF),
            vm((2, ROWS, width), BF), vm((2, ROWS, width), BF), vm((NX, ROWS, width), F32),
        ]
    return pl.pallas_call(
        kernel,
        out_shape=pltpu.VMEM((ROWS, COLS), BF),
        in_specs=[pl.BlockSpec(memory_space=pltpu.HBM)] * 14,
        out_specs=pl.BlockSpec(memory_space=pltpu.VMEM),
        scratch_shapes=scratch,
        compiler_params=pltpu.CompilerParams(
            collective_id=0, has_side_effects=True, vmem_limit_bytes=60 * 1024 * 1024
        ),
        name="layer",
    )(
        inner_pre, coeff_pre, gate_pre, step_raw.T, step_bias[None], decay_log[None], conv_inner,
        conv_coeff, mixer_gain[None], out_weight, residual, mlp_gain[None], up_weight, down_weight.T,
    )


def solution(mesh):
    split = Mesh(mesh.devices.reshape(N, N, NX, 2), ("z", "y", "x", "c"))
    sp, tp = ("z", "y"), ("x", "c")
    return jax.shard_map(
        shards,
        mesh=split,
        in_specs=(
            P(sp, tp), P(sp, None, tp), P(sp, tp), P(sp, tp), P(tp), P(tp), P(None, tp), P(None, None, tp), P(tp),
            P(tp, None), P(sp, tp), P(tp), P(sp, tp), P(tp, sp),
        ),
        out_specs=P(sp, tp),
        check_vma=False,
    )
```

```python
import jax
import jax.numpy as jnp
from jax import lax
from jax.experimental import pallas as pl
from jax.experimental.pallas import tpu as pltpu
from jax.sharding import Mesh
from jax.sharding import PartitionSpec as P

MESH = pl.DeviceIdType.MESH
BF = jnp.bfloat16
F32 = jnp.float32
HIGH = lax.Precision.HIGHEST
EPS = 1e-05

ROWS = 384
HALF = ROWS // 2
BLOCK = 128
NB = ROWS // BLOCK
INNER = 512
STATE = 128
HEADS = 8
COLS = 256
FF = 1024
D = 2048
N = 8
NX = 4
PIECE = 32
SLICE = STATE // N
EDGE = 16


def dot(a, b, dims, precision=None):
    return lax.dot_general(a, b, (dims, ((), ())), precision=precision, preferred_element_type=F32)


NN = ((1,), (0,))
NT = ((1,), (1,))
TN = ((0,), (0,))


def per_head(v):
    low = lax.broadcasted_iota(jnp.int32, (v.shape[0], 128), 1) < 64
    tiles = [jnp.where(low, v[:, 2 * j : 2 * j + 1], v[:, 2 * j + 1 : 2 * j + 2]) for j in range(HEADS // 2)]
    return jnp.concatenate(tiles, axis=1)


def silu(v):
    return v / (1.0 + jnp.exp(-v))


def kernel(
    inner_hbm, coeff_hbm, gate_hbm, step_raw_hbm, step_bias_hbm, decay_log_hbm, taps_inner_hbm, taps_coeff_hbm,
    mixer_gain_hbm, out_hbm, residual_hbm, mlp_gain_hbm, up_hbm, down_hbm, result,
    inner, coeff, gate, residual, up, down, step_raw, step_bias, decay_log, taps_inner, taps_coeff, mixer_gain,
    mlp_gain,
    hist_inner, hist_coeff, ext, ext_c, act, cum, cum_t, step, step_t, local, states, own, enter,
    ld_own, ld_row, ld_total, ld_rows, pre, st_row, st_total, st_rows, st_back,
    mixed, out_w, up_all, down_all, gain_own, gain_all,
    rows, first, acc, active, send, recv, local_sem, tokens, *reductions,
):
    z, y, x, c = (lax.axis_index(a) for a in ("z", "y", "x", "c"))
    tp = 2 * x + c
    at = lambda v, d: lax.rem(v + d, N)
    atx = lambda d: lax.rem(x + d, NX)
    next_id = {"z": at(z, jnp.where(y == N - 1, 1, 0)), "y": at(y, 1)}
    prev_id = {"z": at(z, jnp.where(y == 0, N - 1, 0)), "y": at(y, N - 1)}
    right, left = {"x": atx(1)}, {"x": atx(NX - 1)}
    partner = {"c": 1 - c}
    tp_id = lambda d: {"x": at(tp, d) // 2, "c": lax.rem(at(tp, d), 2)}

    barrier = pltpu.get_barrier_semaphore()
    beside = [{"y": at(y, 1)}, {"y": at(y, N - 1)}, {"z": at(z, 1)}, {"z": at(z, N - 1)}]
    greeted = beside + [right, left, partner, next_id, prev_id]
    for where in greeted:
        pl.semaphore_signal(barrier, inc=1, device_id=where, device_id_type=MESH)

    fetched = [
        pltpu.make_async_copy(there, here, local_sem.at[i])
        for i, (there, here) in enumerate(
            (
                (up_hbm, up), (down_hbm, down), (inner_hbm, inner), (coeff_hbm, coeff), (step_raw_hbm, step_raw),
                (step_bias_hbm, step_bias), (decay_log_hbm, decay_log), (mlp_gain_hbm, mlp_gain),
                (taps_inner_hbm, taps_inner), (taps_coeff_hbm, taps_coeff), (mixer_gain_hbm, mixer_gain),
                (gate_hbm, gate), (residual_hbm, residual), (out_hbm, out_w),
            )
        )
    ]
    for copy in fetched:
        copy.start()
    mixer_gain_copy, gate_copy, residual_copy, out_copy = fetched[10:]

    used = [0, 0]
    pending = []

    def remote(src, dst, where, sent, arrived):
        return pltpu.make_async_remote_copy(
            src_ref=src, dst_ref=dst, send_sem=sent, recv_sem=arrived, device_id=where, device_id_type=MESH
        )

    def sender(total):
        used[0] += 1
        pending.append((send.at[used[0] - 1], total))
        return send.at[used[0] - 1]

    def receiver():
        used[1] += 1
        return recv.at[used[1] - 1]

    def go(*args):
        remote(*args).start()

    def landed(arrived, total):
        remote(total, total, partner, send.at[0], arrived).wait_recv()

    row_i = lax.broadcasted_iota(jnp.int32, (BLOCK, BLOCK), 0)
    col_i = lax.broadcasted_iota(jnp.int32, (BLOCK, BLOCK), 1)
    causal = row_i >= col_i
    tril = causal.astype(F32)
    triu = (row_i <= col_i).astype(F32)
    eye = (row_i == col_i).astype(F32)
    low_lanes = col_i < 64

    seven = pl.ds(0, N - 1)

    def to_all(source, target, where):
        sent, arrived = sender(target[1]), receiver()
        for d in range(1, N):
            go(source(d), target[0], where(d), sent, arrived)
        return lambda: landed(arrived, target[1])

    along_y, along_z = lambda d: {"y": at(y, d)}, lambda d: {"z": at(z, d)}
    OFFSETS = ((0,), (N - 1, 1), (N - 2, 2), (N - 3, 3), (4,))
    weights_sent = [[sender(w.at[0, seven]), sender(w.at[seven])] for w in (up_all, down_all)]
    weights_landed = [
        [[receiver() for _ in range(4)], [[receiver() for _ in range(5)] for _ in range(4)]] for _ in range(2)
    ]

    def forward(weight, stage, way, hop, batch=0, offset=0):
        back = (N - (hop - 1)) % N if way == 0 else hop - 1
        to = 1 if way == 0 else N - 1
        whole, piece = (up_all, up) if weight == 0 else (down_all, down)
        arrived = weights_landed[weight][stage][hop - 1]
        arrived = arrived if stage == 0 else arrived[batch]
        columns = slice(None) if hop < 4 else pl.ds(way * (FF // 2), FF // 2)
        for order in range(2):
            part = pl.ds(order * (PIECE // 2), PIECE // 2)
            a, b = (z, y) if order == 0 else (y, z)
            if stage == 0:
                ia, ib = at(a, back), b
            else:
                ia, ib = at(a, offset), at(b, back)
            on_z = (stage == 0) == (order == 0)
            where = {"z": at(z, to)} if on_z else {"y": at(y, to)}
            iz, iy = (ia, ib) if order == 0 else (ib, ia)
            ref = whole.at[iz, iy, part, columns]
            source = piece.at[part] if hop == 1 and offset == 0 else ref
            go(source, ref, where, weights_sent[weight][stage], arrived)

    def pieces_landed(weight, stage, hop, batch=0):
        count = len(OFFSETS[batch]) * (1 if hop == 4 else 2)
        arrived = weights_landed[weight][stage][hop - 1]
        if stage == 0:
            arrived, count = arrived, 1 if hop == 4 else 2
        else:
            arrived = arrived[batch]
        landed(arrived, (up_all if weight == 0 else down_all).at[0, pl.ds(0, count)])

    def along(weight, hop):
        if hop > 1:
            pieces_landed(weight, 0, hop - 1)
        if hop < 5:
            forward(weight, 0, 0, hop)
            forward(weight, 0, 1, hop)

    def across_to(weight, hop, batch):
        if hop > 1:
            pieces_landed(weight, 1, hop - 1, batch)
        for offset in OFFSETS[batch]:
            forward(weight, 1, 0, hop, batch, offset)
            forward(weight, 1, 1, hop, batch, offset)

    UP = (
        (1, (1, 0)),
        (2, (1, 1)),
        (3, (1, 2), (2, 0)),
        (4, (1, 3), (2, 1)),
        (5, (1, 4), (2, 2), (3, 0)),
        ((2, 3), (3, 1)),
        ((2, 4), (3, 2), (4, 0)),
        ((3, 3), (4, 1)),
        ((3, 4), (4, 2)),
        ((4, 3),),
        ((4, 4),),
    )
    DOWN = (
        (1, (1, 0)),
        (2, (1, 1)),
        (3, (2, 0)),
        ((1, 2), 4, (2, 1)),
        ((1, 3), (3, 0)),
        (5, (1, 4), (2, 2)),
        ((2, 3), (3, 1)),
        ((2, 4),),
        ((3, 2), (3, 3)),
        ((3, 4), (4, 0)),
        ((4, 1), (4, 2)),
        ((4, 3),),
        ((4, 4),),
    )

    def rounds(weight, items):
        for item in items:
            if isinstance(item, int):
                along(weight, item)
            else:
                across_to(weight, *item)

    def event(k):
        rounds(0, UP[k])

    def fill(k):
        rounds(1, DOWN[k])

    for copy in fetched[:4]:
        copy.wait()
    pl.semaphore_wait(barrier, len(greeted))
    inner_tail, coeff_tail = receiver(), receiver()
    go(inner.at[pl.ds(ROWS - EDGE, EDGE)], hist_inner, next_id, sender(hist_inner), inner_tail)
    go(coeff.at[pl.ds(ROWS - 8, 8)], hist_coeff, next_id, sender(hist_coeff), coeff_tail)
    event(0)
    fill(0)

    def pass_tokens(first, targets):
        for i, where in enumerate(targets):
            pl.semaphore_signal(tokens.at[first + i], inc=1, device_id=where, device_id_type=MESH)

    def take_tokens(first):
        for i in range(4):
            pl.semaphore_wait(tokens.at[first + i], 1)

    pass_tokens(0, beside)
    pl.semaphore_signal(tokens.at[4], inc=1, device_id=right, device_id_type=MESH)
    pl.semaphore_signal(tokens.at[5], inc=1, device_id=left, device_id_type=MESH)
    up_all[z, y] = up[...]
    down_all[z, y] = down[...]

    on_heads = lax.broadcasted_iota(jnp.int32, (HEADS, HEADS), 0) == lax.broadcasted_iota(jnp.int32, (HEADS, HEADS), 1)
    column = lambda v: jnp.sum(jnp.where(on_heads, jnp.broadcast_to(v, (HEADS, HEADS)), 0.0), axis=1, keepdims=True)
    for copy in fetched[4:10]:
        copy.wait()
    bias = column(step_bias[...])
    rate = jnp.exp(column(decay_log[...]))
    ends = []
    for b in range(NB):
        rb = pl.ds(b * BLOCK, BLOCK)
        raw = step_raw[:, rb].astype(F32) + bias
        size = jnp.maximum(raw, 0.0) + jnp.log1p(jnp.exp(-jnp.abs(raw)))
        logs = -size * rate
        cum_b = dot(tril, logs, NT, HIGH)
        cum[rb, :] = cum_b
        cum_t[:, rb] = dot(logs, triu, NN, HIGH)
        step[rb, :] = dot(eye, size, NT, HIGH)
        step_t[:, rb] = size
        ends.append(cum_b[BLOCK - 1 : BLOCK, :])
    total = ends[0] + ends[1] + ends[2]
    ld_own[...] = jnp.zeros_like(ld_own)
    ld_own[:, 0:HEADS] = total
    gain_own[...] = jnp.broadcast_to(mlp_gain[...], gain_own.shape)

    ext[8 : 8 + ROWS, :] = inner[...].astype(F32)
    ext_c[8 : 8 + ROWS] = coeff[...].astype(F32)

    ext[0:8, :] = jnp.zeros((8, INNER), F32)
    ext_c[0:8] = jnp.zeros((8, 2, STATE), F32)

    def taps(b, count=BLOCK):
        for j in range(4):
            if j < 2:
                lanes = slice(COLS * j, COLS * (j + 1))
                weights = taps_inner[:, lanes].astype(F32)
                shifted = lambda k: ext[pl.ds(b * BLOCK + 5 + k, count), lanes]
                target = lanes
            else:
                weights = taps_coeff[...].astype(F32)[:, j - 2, :]
                shifted = lambda k: ext_c[pl.ds(b * BLOCK + 5 + k, count), j - 2, :]
                target = slice(INNER + STATE * (j - 2), INNER + STATE * (j - 1))
            total_taps = shifted(0) * weights[0:1]
            for k in range(1, 4):
                total_taps = total_taps + shifted(k) * weights[k : k + 1]
            act[b * BLOCK : b * BLOCK + count, target] = silu(total_taps).astype(BF)

    def block_state(b):
        rb = slice(b * BLOCK, (b + 1) * BLOCK)
        weight = step[rb, :] * jnp.exp(ends[b] - cum[rb, :])
        values = act[rb, 0:INNER].astype(F32) * per_head(weight)
        states[b] = dot(act[rb, INNER : INNER + STATE], values.astype(BF), TN)

    taps(1)
    block_state(1)
    take_tokens(0)
    pass_tokens(7, [{"y": at(y, 2)}, {"y": at(y, N - 2)}, {"z": at(z, 2)}, {"z": at(z, N - 2)}])
    pl.semaphore_wait(tokens.at[4], 1)
    pl.semaphore_wait(tokens.at[5], 1)
    pl.semaphore_signal(tokens.at[6], inc=1, device_id=partner, device_id_type=MESH)
    taps(2)
    block_state(2)
    taps(0)
    landed(inner_tail, hist_inner)
    landed(coeff_tail, hist_coeff)
    is_first = jnp.logical_and(z == 0, y == 0)
    ext[0:8, :] = jnp.where(is_first, 0.0, hist_inner[8:16, :].astype(F32))
    ext_c[0:8] = jnp.where(is_first, 0.0, hist_coeff[...].astype(F32))
    taps(0, EDGE)
    block_state(0)
    own[...] = (
        states[0] * per_head(jnp.exp(ends[1] + ends[2])) + states[1] * per_head(jnp.exp(ends[2])) + states[2]
    ).astype(BF)

    slice_of = lambda v: pl.ds(pl.multiple_of(v * SLICE, SLICE), SLICE)
    take_tokens(7)
    pl.semaphore_wait(tokens.at[6], 1)
    ld_landed = to_all(lambda d: ld_own, (ld_row.at[y], ld_row.at[seven]), along_y)
    ld_row[y] = ld_own[...]
    st1_landed = to_all(lambda d: own.at[slice_of(at(y, d))], (st_row.at[y], st_row.at[seven]), along_y)
    event(1)
    fill(1)
    st_row[y] = own[slice_of(y), :]

    def inside(b):
        rb = slice(b * BLOCK, (b + 1) * BLOCK)
        scores = dot(act[rb, INNER + STATE :], act[rb, INNER : INNER + STATE], NT)
        for j in range(HEADS // 2):
            lanes = slice(128 * j, 128 * (j + 1))
            parts = []
            for h in (2 * j, 2 * j + 1):
                gap = cum[rb, h : h + 1] - cum_t[h : h + 1, rb]
                within = jnp.exp(jnp.where(causal, gap, -1e30)) * (scores * step_t[h : h + 1, rb])
                parts.append(dot(within.astype(BF), act[rb, lanes], NN))
            local[rb, lanes] = jnp.where(low_lanes, parts[0], parts[1])

    def carried(b):
        rb = slice(b * BLOCK, (b + 1) * BLOCK)
        if b == 1:
            inner_state = states[0]
        else:
            inner_state = states[0] * per_head(jnp.exp(ends[1])) + states[1]
        local[rb, :] += dot(act[rb, INNER + STATE :], inner_state.astype(BF), NN) * per_head(jnp.exp(cum[rb, :]))

    gain_landed = to_all(lambda d: gain_own, (gain_all.at[tp], gain_all.at[seven]), tp_id)
    gain_all[tp] = gain_own[...]
    ld_landed()
    row_logs = ld_row[:, 0, :]
    ld_total[...] = jnp.sum(row_logs, axis=0, keepdims=True)
    ld2_landed = to_all(lambda d: ld_total, (ld_rows.at[z], ld_rows.at[seven]), along_z)
    ld_rows[z] = ld_total[...]
    row_decay = per_head(jnp.exp(row_logs))

    inside(0)
    inside(1)
    inside(2)
    carried(1)
    carried(2)
    st1_landed()
    run = jnp.zeros((SLICE, INNER), F32)
    for k in range(N):
        pre[k] = run
        run = run * row_decay[k : k + 1, :] + st_row[k].astype(F32)
    st_total[...] = run.astype(BF)
    st2_landed = to_all(lambda d: st_total, (st_rows.at[z], st_rows.at[seven]), along_z)
    st_rows[z] = st_total[...]
    event(2)
    fill(2)
    ld2_landed()
    rows_decay = per_head(jnp.exp(ld_rows[:, 0, :]))
    st2_landed()
    run = jnp.zeros((SLICE, INNER), F32)
    for k in range(N):
        run = jnp.where(k < z, run * rows_decay[k : k + 1, :] + st_rows[k].astype(F32), run)
    for k in range(N):
        st_back[k] = (pre[k] + run).astype(BF)
        if k < N - 1:
            run = run * row_decay[k : k + 1, :]
    st3_landed = to_all(
        lambda d: st_back.at[at(y, d)], (enter.at[slice_of(y)], enter.at[pl.ds(0, SLICE * (N - 1))]), along_y
    )
    enter[slice_of(y), :] = st_back[y]

    event(3)
    fill(3)
    st3_landed()
    event(4)
    fill(4)
    mixer_gain_copy.wait()
    gate_copy.wait()
    start_log = jnp.zeros_like(ends[0])
    for b in range(NB):
        rb = slice(b * BLOCK, (b + 1) * BLOCK)
        outer = dot(act[rb, INNER + STATE :], enter[...], NN) * per_head(jnp.exp(cum[rb, :] + start_log))
        gated = (local[rb, :] + outer) * silu(gate[rb, :].astype(F32))
        mean = jnp.mean(gated * gated, axis=1, keepdims=True)
        mixed[rb, :] = (gated * lax.rsqrt(mean + EPS) * mixer_gain[...]).astype(BF)
        start_log = start_log + ends[b]

    top, bottom = pl.ds(0, HALF), pl.ds(HALF, HALF)

    class Reduction:
        def __init__(self, block, refs):
            self.block = block
            self.pair_out, self.pair_in, self.far, self.relay, self.near, self.fin, self.keep = refs
            self.pair_sent, self.ring_sent = sender(self.pair_in), sender(self.pair_in.at[pl.ds(0, 3)])
            self.pair_landed = [receiver() for _ in range(NX)]
            self.from_l, self.from_r, self.final = receiver(), receiver(), receiver()

        def both(self, *members):
            value = self.block(*[atx((2, 1, 3, 0)[i]) for i in members])
            width = value.shape[1] // len(members)
            for n, i in enumerate(members):
                self.share(i, value[:, n * width : (n + 1) * width])

        def share(self, i, value):
            width = value.shape[1] // 2
            lower, upper = value[:, :width], value[:, width:]
            self.pair_out[i] = jnp.where(c == 0, upper, lower).astype(BF)
            go(self.pair_out.at[i], self.pair_in.at[i], partner, self.pair_sent, self.pair_landed[i])
            self.keep[i] = jnp.where(c == 0, lower, upper)

        def mine(self, i):
            landed(self.pair_landed[i], self.pair_in.at[i])
            return self.keep[i] + self.pair_in[i].astype(F32)

        def send_far(self):
            self.far[...] = self.mine(0).astype(BF)
            go(self.far.at[top], self.relay.at[0], right, self.ring_sent, self.from_l)
            go(self.far.at[bottom], self.relay.at[1], left, self.ring_sent, self.from_r)

        def send_right(self):
            self.keep[1] = value = self.mine(1)
            self.near[0, HALF:, :] = value[HALF:].astype(BF)
            go(self.near.at[0, bottom], self.fin.at[0, bottom], right, self.ring_sent, self.final)

        def send_left(self):
            self.keep[2] = value = self.mine(2)
            self.near[1, :HALF, :] = value[:HALF].astype(BF)
            go(self.near.at[1, top], self.fin.at[1, top], left, self.ring_sent, self.final)

        def own(self):
            self.keep[3] = self.mine(3)

        def pass_on(self):
            landed(self.from_l, self.relay.at[0])
            self.near[0, :HALF, :] = (self.keep[1, :HALF, :] + self.relay[0].astype(F32)).astype(BF)
            go(self.near.at[0, top], self.fin.at[0, top], right, self.ring_sent, self.final)
            landed(self.from_r, self.relay.at[1])
            self.near[1, HALF:, :] = (self.keep[2, HALF:, :] + self.relay[1].astype(F32)).astype(BF)
            go(self.near.at[1, bottom], self.fin.at[1, bottom], left, self.ring_sent, self.final)

        def total(self):
            landed(self.final, self.fin)
            return self.keep[3] + self.fin[0].astype(F32) + self.fin[1].astype(F32)

    def out_block(chip):
        return dot(mixed[...], out_w[:, pl.ds(pl.multiple_of(chip * 2 * COLS, 2 * COLS), 2 * COLS)], NN)

    out_copy.wait()
    mixer_sum = Reduction(out_block, reductions[0:7])
    mixer_sum.both(0)
    mixer_sum.both(1)
    mixer_sum.send_far()
    mixer_sum.both(2)
    mixer_sum.send_right()
    mixer_sum.both(3)
    mixer_sum.send_left()
    mixer_sum.own()
    event(5)
    fill(5)
    mixer_sum.pass_on()
    event(6)
    fill(6)
    projected = mixer_sum.total()
    residual_copy.wait()
    first[...] = (residual[...].astype(F32) + projected).astype(BF)
    rows[tp] = first[...]

    mine_tp, left_tp, right_tp, far_tp = tp, 2 * atx(3) + c, 2 * atx(1) + c, 2 * atx(2) + c
    rows_sent = sender(rows.at[seven])
    l_first, r_first, l_second, r_second, far_landed, across_landed = (receiver() for _ in range(6))
    go(first.at[top], rows.at[tp, top], right, rows_sent, l_first)
    go(first.at[bottom], rows.at[tp, bottom], left, rows_sent, r_first)
    go(first, rows.at[tp], partner, rows_sent, across_landed)
    go(first.at[bottom], rows.at[tp, bottom], right, rows_sent, l_second)
    go(first.at[top], rows.at[tp, top], left, rows_sent, r_second)
    event(7)
    fill(7)
    gain_landed()
    squares = jnp.zeros((ROWS, 1), F32)

    def raise_rows(source, squares, new=False):
        wide = rows[source].astype(F32)
        squares = squares + jnp.sum(wide * wide, axis=1, keepdims=True)
        scaled = (wide * gain_all[source][0:1, :]).astype(BF)
        weights = up_all[source].reshape(COLS, FF)
        product = dot(scaled, weights, NN)
        acc[...] = product if new else acc[...] + product
        return squares

    half_rows = rows.at[0, top]
    landed(l_first, half_rows)
    go(rows.at[left_tp, top], rows.at[left_tp, top], right, rows_sent, far_landed)
    landed(r_first, half_rows)
    go(rows.at[right_tp, bottom], rows.at[right_tp, bottom], left, rows_sent, far_landed)
    event(8)
    fill(8)
    landed(l_second, half_rows)
    go(rows.at[left_tp], rows.at[left_tp], partner, rows_sent, across_landed)
    landed(r_second, half_rows)
    go(rows.at[right_tp], rows.at[right_tp], partner, rows_sent, across_landed)
    event(9)
    landed(far_landed, rows.at[0])
    go(rows.at[far_tp], rows.at[far_tp], partner, rows_sent, across_landed)
    event(10)
    fill(9)
    fill(10)
    landed(across_landed, rows.at[pl.ds(0, NX)])
    fill(11)
    for batch in range(5):
        pieces_landed(0, 1, 4, batch)
    for k in range(N):
        squares = raise_rows(k, squares, k == 0)
        if k == 2:
            fill(12)
    scale = lax.rsqrt(squares * (1.0 / D) + EPS)
    active[...] = jnp.square(jnp.maximum(acc[...] * scale, 0.0)).astype(BF)

    def down_block(half):
        def block(*chips):
            pieces = [
                down_all[2 * chip + j, at(y, (N - 1 + 4 * half + p) % N)]
                for chip in chips
                for j in range(2)
                for p in range(4)
            ]
            return dot(active[...], jnp.concatenate(pieces, axis=0), NT)

        return block

    early, late = Reduction(down_block(0), reductions[7:14]), Reduction(down_block(1), reductions[14:21])
    for batch in range(3):
        pieces_landed(1, 1, 4, batch)
    early.both(0, 1)
    early.both(2, 3)
    early.send_far()
    early.send_right()
    early.send_left()
    for batch in range(3, 5):
        pieces_landed(1, 1, 4, batch)
    late.both(0, 1)
    early.own()
    late.both(2, 3)
    late.send_far()
    early.pass_on()
    late.send_right()
    late.send_left()
    late.own()
    late.pass_on()
    turned = early.total()
    turned = jnp.concatenate([turned, late.total()], axis=1)
    lowered = pltpu.roll(turned, at(y, N - 1) * PIECE, 1)
    result[...] = (first[...].astype(F32) + lowered).astype(BF)
    for sent, total in pending:
        remote(total, total, partner, sent, recv.at[0]).wait_send()


def shards(
    inner_pre, coeff_pre, gate_pre, step_raw, step_bias, decay_log, conv_inner, conv_coeff, mixer_gain,
    out_weight, residual, mlp_gain, up_weight, down_weight,
):
    vm = pltpu.VMEM
    dma = pltpu.SemaphoreType.DMA
    scratch = [
        vm((ROWS, INNER), BF), vm((ROWS, 2, STATE), BF), vm((ROWS, INNER), BF), vm((ROWS, COLS), BF),
        vm((PIECE, FF), BF), vm((PIECE, FF), BF), vm((HEADS, ROWS), BF), vm((1, HEADS), F32), vm((1, HEADS), F32),
        vm((4, INNER), BF), vm((4, 2, STATE), BF), vm((1, INNER), F32), vm((1, COLS), F32),
        vm((EDGE, INNER), BF), vm((8, 2, STATE), BF), vm((ROWS + 8, INNER), F32), vm((ROWS + 8, 2, STATE), F32), vm((ROWS, INNER + COLS), BF),
        vm((ROWS, HEADS), F32), vm((HEADS, ROWS), F32), vm((ROWS, HEADS), F32), vm((HEADS, ROWS), F32),
        vm((ROWS, INNER), F32), vm((NB, STATE, INNER), F32), vm((STATE, INNER), BF), vm((STATE, INNER), BF),
        vm((1, 128), F32), vm((N, 1, 128), F32), vm((1, 128), F32), vm((N, 1, 128), F32),
        vm((N, SLICE, INNER), F32), vm((N, SLICE, INNER), BF), vm((SLICE, INNER), BF), vm((N, SLICE, INNER), BF),
        vm((N, SLICE, INNER), BF),
        vm((ROWS, INNER), BF), vm((INNER, D), BF), vm((N, N, PIECE, FF), BF), vm((N, N, PIECE, FF), BF),
        vm((8, COLS), F32), vm((N, 8, COLS), F32),
        vm((N, ROWS, COLS), BF), vm((ROWS, COLS), BF), vm((ROWS, FF), F32), vm((ROWS, FF), BF),
        dma((19,)), dma((83,)), dma((14,)), pltpu.SemaphoreType.REGULAR((11,)),
    ]
    for width in (COLS, COLS // 2, COLS // 2):
        scratch += [
            vm((NX, ROWS, width), BF), vm((NX, ROWS, width), BF), vm((ROWS, width), BF), vm((2, HALF, width), BF),
            vm((2, ROWS, width), BF), vm((2, ROWS, width), BF), vm((NX, ROWS, width), F32),
        ]
    return pl.pallas_call(
        kernel,
        out_shape=pltpu.VMEM((ROWS, COLS), BF),
        in_specs=[pl.BlockSpec(memory_space=pltpu.HBM)] * 14,
        out_specs=pl.BlockSpec(memory_space=pltpu.VMEM),
        scratch_shapes=scratch,
        compiler_params=pltpu.CompilerParams(
            collective_id=0, has_side_effects=True, vmem_limit_bytes=60 * 1024 * 1024
        ),
        name="layer",
    )(
        inner_pre, coeff_pre, gate_pre, step_raw.T, step_bias[None], decay_log[None], conv_inner,
        conv_coeff, mixer_gain[None], out_weight, residual, mlp_gain[None], up_weight, down_weight.T,
    )


def solution(mesh):
    split = Mesh(mesh.devices.reshape(N, N, NX, 2), ("z", "y", "x", "c"))
    sp, tp = ("z", "y"), ("x", "c")
    return jax.shard_map(
        shards,
        mesh=split,
        in_specs=(
            P(sp, tp), P(sp, None, tp), P(sp, tp), P(sp, tp), P(tp), P(tp), P(None, tp), P(None, None, tp), P(tp),
            P(tp, None), P(sp, tp), P(tp), P(sp, tp), P(tp, sp),
        ),
        out_specs=P(sp, tp),
        check_vma=False,
    )
```
